32 devices in a mesh: grp: 2 (over y), sp: 4 (over z), tp: 4 (over x, core).
Axes of the slice: x: 2, y: 2, z: 4, core: 2. Of those that a mesh axis runs over, the one named last changes fastest.
Arguments:
- query_rows: bfloat16 [4096, 1024], P(('grp', 'sp'), 'tp'), parts along dimension 0, may hold values from -128 to 128
- key_rows: bfloat16 [4096, 256], P(('grp', 'sp'), 'tp'), parts along dimension 0, may hold values from -4 to 4
- value_rows: bfloat16 [4096, 256], P(('grp', 'sp'), 'tp'), parts along dimension 0, may hold values from -6 to 6
- sink_logits: float32 [16], P('tp'), may hold values from 3 to 7
- residual: bfloat16 [4096, 2048], P(('grp', 'sp', 'tp')), parts along dimension 0, may hold values from -6 to 6
- out_weight: bfloat16 [1024, 2048], P('tp'), may hold values from -0.1875 to 0.1875
- norm_gain: float32 [2048], replicated, may hold values from 0.1 to 1.9
- gate_weight: bfloat16 [16, 2048, 512], P(('sp', 'tp')), may hold values from -0.125 to 0.125
- up_weight: bfloat16 [16, 2048, 512], P(('sp', 'tp')), may hold values from -0.125 to 0.125
- down_weight: bfloat16 [16, 512, 2048], P(('sp', 'tp')), may hold values from -0.25 to 0.25
- routes: int32 [4096, 2], P(('grp', 'sp', 'tp')), parts along dimension 0, may hold values from 0 to 15, as said below
- route_weight: float32 [4096, 2], P(('grp', 'sp', 'tp')), parts along dimension 0, may hold values from 0.1 to 1
Outputs:
- layer_out: bfloat16 [4096, 2048], P(('grp', 'sp', 'tp')), parts along dimension 0
The draws below stay inside these ranges and needn't reach their ends.
There are 2 independent parts, one for each index of `grp`. The reference program is written for one: setup_inputs(seed, part) draws one part's arguments, and reference() takes and returns one part's arrays. A program takes and returns all parts, laid end to end along the dimension named above; an argument that names none is the same for every part. Nothing has to cross between parts.
Inputs may be any that keep to these rules, and one draw needn't show every extreme that they name: `routes`: A token's two experts differ and lie in the same group of 4 consecutive experts. Among the 128 tokens of one device (aligned blocks of 128 rows) no expert is named more than 32 times; in every block each expert of one group, the same group for all blocks, is named exactly 32 times.
All inputs are finite; a program needn't handle non-finite values.
Results may differ from the reference program's by a relative error of at most 0.013.
Values may be sent and summed in bfloat16 or wider, within the bound.
A program may use at most 64 MiB of HBM per device.

```python
import math
import jax
import jax.numpy as jnp
from jax import lax

D = 2048
HEADS = 16
KV = 4
HDIM = 64
WINDOW = 128
FFE = 512
GROUPS = 4
TOKENS = 2048
ROWS = 128
EXPERTS = 16
EPG = 4
CAP = 32


def shared_rows(key):
    key_part = jnp.clip(jax.random.normal(jax.random.fold_in(key, 1), (TOKENS, KV * HDIM), jnp.float32), -4.0, 4.0)
    query_part = jnp.clip(jax.random.normal(jax.random.fold_in(key, 2), (TOKENS, HEADS * HDIM), jnp.float32), -4.0, 4.0)
    return (query_part, key_part)


def draw_query_rows(key, part):
    query_part, key_part = shared_rows(jax.random.fold_in(key, 17))
    return query_part.astype(jnp.bfloat16)


def draw_key_rows(key, part):
    query_part, key_part = shared_rows(jax.random.fold_in(key, 17))
    return key_part.astype(jnp.bfloat16)


def draw_routes(key, part):
    block_count = TOKENS // ROWS
    half_rows = ROWS // 2
    full_group = jax.random.randint(jax.random.fold_in(key, 5), (), 0, GROUPS)

    def one_block(block_key):
        cuts = jnp.sort(jax.random.randint(jax.random.fold_in(block_key, 1), (GROUPS - 2,), 0, half_rows + 1))
        bounds = jnp.concatenate([jnp.zeros((1,), jnp.int32), cuts.astype(jnp.int32), jnp.full((1,), half_rows, jnp.int32)])
        other_sizes = bounds[1:] - bounds[:-1]
        others = (full_group + 1 + jnp.arange(GROUPS - 1, dtype=jnp.int32)) % GROUPS
        sizes = jnp.zeros((GROUPS,), jnp.int32).at[others].set(other_sizes).at[full_group].set(half_rows)
        ends = jnp.cumsum(sizes)
        starts = ends - sizes
        order = jax.random.permutation(jax.random.fold_in(block_key, 2), ROWS)
        places = jnp.arange(ROWS, dtype=jnp.int32)
        group_of = jnp.sum((places[:, None] >= ends[None, :]).astype(jnp.int32), axis=1)
        within = places - starts[group_of]
        group_keys = jax.vmap(lambda g: jax.random.fold_in(block_key, 10 + g))(jnp.arange(GROUPS, dtype=jnp.int32))
        perms = jax.vmap(lambda k: jax.random.permutation(k, EPG))(group_keys).astype(jnp.int32)
        offset = 1 + within // EPG % (EPG - 1)
        first_local = perms[group_of, within % EPG]
        second_local = perms[group_of, (within + offset) % EPG]
        pair = jnp.stack([group_of * EPG + first_local, group_of * EPG + second_local], axis=1).astype(jnp.int32)
        return jnp.zeros((ROWS, 2), jnp.int32).at[order].set(pair)
    block_keys = jax.vmap(lambda b: jax.random.fold_in(key, 100 + b))(jnp.arange(block_count, dtype=jnp.int32))
    return jax.vmap(one_block)(block_keys).reshape(TOKENS, 2)


def block_levels(own_key, extent, split, smallest, top_value):
    def one(axis_at, blocks):
        heights = jax.random.uniform(jax.random.fold_in(jax.random.fold_in(own_key, 6), axis_at), (blocks,), jnp.float32, smallest / len(split), top_value / len(split))
        return jnp.repeat(jnp.exp(heights), extent[axis_at] // blocks).reshape((-1,) + (1,) * (len(extent) - axis_at - 1))

    level = one(*split[0])
    for cut in split[1:]:
        level = level * one(*cut)
    return level


def normal_values(own_key, extent, scale, limit, shards=(), kind=jnp.bfloat16):
    entries = scale * jax.random.normal(own_key, extent, jnp.float32)
    if shards:
        entries = entries * block_levels(own_key, extent, shards, -0.22, 0.18)
    return jnp.clip(entries, -limit, limit).astype(kind)


def setup_inputs(seed: int = 0, part: int = 0) -> dict:
    keys = jax.random.split(jax.random.key(seed), 13)
    part_splits = jax.random.split(jax.random.fold_in(keys[12], part), 13)
    query_rows = draw_query_rows(jax.random.fold_in(jax.random.fold_in(keys[12], part), 71), part)
    key_rows = draw_key_rows(jax.random.fold_in(jax.random.fold_in(keys[12], part), 71), part)
    value_rows = normal_values(part_splits[2], (TOKENS, KV * HDIM), 1.0, 6.0, ((0, 4), (1, 4)))
    sink_logits = jnp.clip(3.0 + 4.0 * jax.random.uniform(keys[3], (HEADS,), jnp.float32) ** block_levels(keys[3], (HEADS,), ((0, 4),), -0.2, 0.2), 3.0, 7.0)
    residual = normal_values(part_splits[4], (TOKENS, D), 1.0, 6.0, ((0, 16),))
    out_weight = normal_values(keys[5], (HEADS * HDIM, D), (HEADS * HDIM) ** -0.5, 0.1875, ((0, 4),))
    norm_gain = jnp.clip(1.0 + 0.18 * jax.random.normal(keys[6], (D,), jnp.float32), 0.1, 1.9)
    gate_weight = normal_values(keys[7], (EXPERTS, D, FFE), D ** -0.5, 0.125, ((0, 16),))
    up_weight = normal_values(keys[8], (EXPERTS, D, FFE), D ** -0.5, 0.125, ((0, 16),))
    down_weight = normal_values(keys[9], (EXPERTS, FFE, D), FFE ** -0.5, 0.25, ((0, 16),))
    routes = draw_routes(jax.random.fold_in(jax.random.fold_in(keys[12], part), 71), part)
    route_weight = jnp.clip(jnp.exp(math.log(1.0) - 2.3025851 * jax.random.uniform(part_splits[11], (TOKENS, 2), jnp.float32) ** block_levels(part_splits[11], (TOKENS, 2), ((0, 16),), -0.2, 0.2)), 0.1, 1.0)
    return {"query_rows": query_rows, "key_rows": key_rows, "value_rows": value_rows, "sink_logits": sink_logits, "residual": residual, "out_weight": out_weight, "norm_gain": norm_gain, "gate_weight": gate_weight, "up_weight": up_weight, "down_weight": down_weight, "routes": routes, "route_weight": route_weight}


rope_base = 10000.0
norm_eps = 1e-06

def rotate(rows, positions, heads):
    half_dim = HDIM // 2
    values = rows.astype(jnp.float32).reshape(rows.shape[0], heads, HDIM)
    inverse = rope_base ** (-jnp.arange(half_dim, dtype=jnp.float32) / half_dim)
    angles = positions.astype(jnp.float32)[:, None] * inverse[None, :]
    cosines = jnp.cos(angles)[:, None, :]
    sines = jnp.sin(angles)[:, None, :]
    lower = values[..., :half_dim]
    upper = values[..., half_dim:]
    turned = jnp.concatenate([lower * cosines - upper * sines, upper * cosines + lower * sines], axis=-1)
    return turned.reshape(rows.shape[0], heads * HDIM).astype(jnp.bfloat16)

def reference(query_rows, key_rows, value_rows, sink_logits, residual, out_weight, norm_gain, gate_weight, up_weight, down_weight, routes, route_weight):
    positions = jnp.arange(TOKENS, dtype=jnp.int32)
    rot_q = rotate(query_rows, positions, HEADS)
    rot_k = rotate(key_rows, positions, KV)
    repeat = HEADS // KV
    blocks = TOKENS // WINDOW
    q_blocks = rot_q.reshape(blocks, WINDOW, KV, repeat, HDIM)
    k_blocks = rot_k.reshape(blocks, WINDOW, KV, HDIM)
    v_blocks = value_rows.reshape(blocks, WINDOW, KV, HDIM)
    k_wide = jnp.concatenate([jnp.concatenate([jnp.zeros_like(k_blocks[:1]), k_blocks[:-1]], axis=0), k_blocks], axis=1)
    v_wide = jnp.concatenate([jnp.concatenate([jnp.zeros_like(v_blocks[:1]), v_blocks[:-1]], axis=0), v_blocks], axis=1)
    query_pos = jnp.arange(WINDOW) + WINDOW
    key_pos = jnp.arange(2 * WINDOW)
    distance = query_pos[:, None] - key_pos[None, :]
    in_band = (distance >= 0) & (distance < WINDOW)
    earliest = (jnp.arange(blocks)[:, None, None] > 0) | (key_pos[None, None, :] >= WINDOW)
    allowed = in_band[None] & earliest
    sinks_grouped = sink_logits.astype(jnp.float32).reshape(KV, repeat)

    def one_group(group):
        q_group = q_blocks[:, :, group].astype(jnp.float32)
        k_group = k_wide[:, :, group].astype(jnp.float32)
        v_group = v_wide[:, :, group].astype(jnp.float32)
        scores = jnp.einsum('nqrd,nkd->rnqk', q_group, k_group) * HDIM ** (-0.5)
        scores = jnp.where(allowed[None], scores, -jnp.inf)
        sink_here = sinks_grouped[group][:, None, None, None]
        largest = jnp.maximum(scores.max(axis=-1, keepdims=True), sink_here)
        exp_scores = jnp.exp(scores - largest)
        denominator = exp_scores.sum(axis=-1, keepdims=True) + jnp.exp(sink_here - largest)
        probs = (exp_scores / denominator).astype(jnp.bfloat16)
        mixed = jnp.einsum('rnqk,nkd->nqrd', probs.astype(jnp.float32), v_group)
        return mixed.astype(jnp.bfloat16)
    attended = lax.map(one_group, jnp.arange(KV, dtype=jnp.int32))
    attended = attended.transpose(1, 2, 0, 3, 4).reshape(TOKENS, HEADS * HDIM)
    projected = jnp.dot(attended, out_weight, preferred_element_type=jnp.float32)
    stream = (residual.astype(jnp.float32) + projected).astype(jnp.bfloat16)
    stream_f = stream.astype(jnp.float32)
    normed = (stream_f * lax.rsqrt(lax.optimization_barrier(jnp.mean(stream_f * stream_f, axis=-1, keepdims=True)) + norm_eps) * norm_gain[None, :]).astype(jnp.bfloat16)
    flat_expert = routes.reshape(-1).astype(jnp.int32)
    token_of = (jnp.arange(2 * TOKENS, dtype=jnp.int32) // 2).astype(jnp.int32)
    one_hot = (flat_expert[:, None] == jnp.arange(EXPERTS, dtype=jnp.int32)[None, :]).astype(jnp.int32)
    slot_rank = lax.optimization_barrier(jnp.sum((jnp.cumsum(one_hot, axis=0) - one_hot) * one_hot, axis=1)).astype(jnp.int32)
    slots = EXPERTS * CAP
    index_table = jnp.full((EXPERTS, slots), TOKENS, jnp.int32).at[flat_expert, slot_rank].set(token_of)
    weight_table = jnp.zeros((EXPERTS, slots), jnp.float32).at[flat_expert, slot_rank].set(route_weight.reshape(-1).astype(jnp.float32))
    padded = jnp.concatenate([normed, jnp.zeros((1, D), jnp.bfloat16)], axis=0)

    def serve(total, expert):
        picked = index_table[expert]
        routed = padded[picked]
        gate_out = jnp.dot(routed, gate_weight[expert], preferred_element_type=jnp.float32)
        up_out = jnp.dot(routed, up_weight[expert], preferred_element_type=jnp.float32)
        hidden = (jax.nn.silu(gate_out) * up_out).astype(jnp.bfloat16)
        expert_out = jnp.dot(hidden, down_weight[expert], preferred_element_type=jnp.float32).astype(jnp.bfloat16)
        total = total.at[picked].add(weight_table[expert][:, None] * expert_out.astype(jnp.float32))
        return (total, None)
    summed, _ = lax.scan(serve, jnp.zeros((TOKENS + 1, D), jnp.float32), jnp.arange(EXPERTS, dtype=jnp.int32))
    return (stream_f + summed[:TOKENS]).astype(jnp.bfloat16)
```

```python
import functools

import jax
import jax.numpy as jnp
from jax import lax
from jax.experimental import pallas as pl
from jax.experimental.pallas import tpu as pltpu
from jax.sharding import PartitionSpec as P

HDIM = 64
WINDOW = 128
GROUPS = 4
MESH = pl.DeviceIdType.MESH


rope_base = 10000.0
norm_eps = 1e-06


def shifted(block, axis, distance):
    devices = range(lax.axis_size(axis))
    route = [(i - distance, i) for i in devices if i - distance in devices]
    return lax.ppermute(block, axis, route)


def rotate(rows, positions, heads):
    half_dim = HDIM // 2
    values = rows.astype(jnp.float32).reshape(rows.shape[0], heads, HDIM)
    inverse = rope_base ** (-jnp.arange(half_dim, dtype=jnp.float32) / half_dim)
    angles = positions.astype(jnp.float32)[:, None] * inverse[None, :]
    cosines = jnp.cos(angles)[:, None, :]
    sines = jnp.sin(angles)[:, None, :]
    lower = values[..., :half_dim]
    upper = values[..., half_dim:]
    turned = jnp.concatenate(
        [lower * cosines - upper * sines, upper * cosines + lower * sines], axis=-1
    )
    return turned.reshape(rows.shape[0], heads * HDIM).astype(jnp.bfloat16)


ORDER = (0, 2, 1, 3)
PIECES = 4
EARLY = 2
PARTS = 2


def layer_kernel(
    q_ref, k_ref, v_ref, inv_ref, sink_ref, w_ref, res_ref, gain_ref, routes_t_ref, rw_t_ref, gate_ref, up_ref,
    down_ref, out_ref,
    wbuf, abuf, acc, xs, rres, aps, rat, own_r, own_a, acc0, tok, gate_v, up_v, down_v, hid, y, yr, sum0, sum2, xrec, zsend, zrec,
    meta, meta_rx, pt_ref, stream_v, kv, rq, heads_v, cos_ref, sin_ref,
    lsem, wss, wrs, kss, krs, ass_, ars, mss, mrs, zss, zrs, oss, ors, dss, drs, rss, rrs,
):
    grp = lax.axis_index("grp")
    sp = lax.axis_index("sp")
    tp = lax.axis_index("tp")
    n_sp = GROUPS
    n_tp = 4
    rows = res_ref.shape[0]
    width = res_ref.shape[1]
    cap = xs.shape[1]
    epg = n_tp
    ff = gate_ref.shape[1]

    def sp_at(d):
        return lax.rem(sp + d, n_sp)

    near = tp + 1 - 2 * lax.rem(tp, 2)

    def tp_at(k):
        base = near if k % 2 else tp
        return lax.rem(base + 2, n_tp) if k >= 2 else base

    depth = w_ref.shape[0]

    def w_at(k):
        return wbuf.at[pl.ds(k * depth, depth)]

    local = [
        pltpu.make_async_copy(w_ref, w_at(0), lsem.at[0]),
        pltpu.make_async_copy(gate_ref, gate_v, lsem.at[1]),
        pltpu.make_async_copy(up_ref, up_v, lsem.at[2]),
        pltpu.make_async_copy(down_ref, down_v, lsem.at[3]),
    ]
    for c in local:
        c.start()

    barrier = pltpu.get_barrier_semaphore()
    for d in range(n_sp):
        for k in range(n_tp):
            if d or k:
                pl.semaphore_signal(
                    barrier, inc=1, device_id={"sp": sp_at(d), "tp": tp_at(k)},
                    device_id_type=MESH,
                )
    pl.semaphore_signal(
        barrier, inc=1, device_id={"grp": 1 - grp}, device_id_type=MESH
    )

    f32 = jnp.float32
    bf = jnp.bfloat16
    toks = q_ref.shape[0]
    half_dim = HDIM // 2
    lane_t = lax.broadcasted_iota(jnp.int32, (toks, 128), 1)
    lower = lax.rem(lane_t, HDIM) < half_dim

    def turn(x):
        other = jnp.where(
            lower, pltpu.roll(x, 128 - half_dim, 1), pltpu.roll(x, half_dim, 1)
        )
        return x * cos_ref[...] + other * sin_ref[...]

    pos = lax.broadcasted_iota(jnp.int32, (toks, 128), 0) + sp * toks
    angle = pos.astype(f32) * inv_ref[...]
    cos_ref[...] = jnp.cos(angle)
    sines = jnp.sin(angle)
    sin_ref[...] = jnp.where(lower, -sines, sines)
    both = jnp.concatenate([k_ref[...], v_ref[...]], axis=0).T
    turned = turn(both.astype(f32)).astype(bf)
    kv[WINDOW:, :] = jnp.where(lane_t < HDIM, turned, both)
    pl.semaphore_wait(barrier, n_sp * n_tp)

    sends = []

    def post(src, dst, ssem, rsem, where):
        c = pltpu.make_async_remote_copy(
            src_ref=src, dst_ref=dst, send_sem=ssem, recv_sem=rsem,
            device_id=where, device_id_type=MESH,
        )
        c.start()
        sends.append(c)
        return c

    def send(src, dst, ssem, rsem, d, k):
        return post(src, dst, ssem, rsem, {"sp": sp_at(d), "tp": tp_at(k)})

    tail = send(kv.at[pl.ds(toks, WINDOW)], kv.at[pl.ds(0, WINDOW)], kss, krs, 1, 0)
    chunk = depth // (2 * PIECES)

    def w_rows(k, half, c):
        return pl.ds(pl.multiple_of(k * depth + half * (depth // 2) + c * chunk, chunk), chunk)

    w_far = []

    def w_open(c):
        w_far.append(
            send(
                w_ref.at[w_rows(0, grp, c)], wbuf.at[w_rows(2, grp, c)], wss.at[0, c], wrs.at[0, c], 0, 2
            )
        )

    w_side, w_last = [], []

    def w_cross(c):
        w_far[c].wait_recv()
        mine = wbuf.at[w_rows(2, grp, c)]
        w_side.append(post(mine, mine, wss.at[1, c], wrs.at[1, c], {"grp": 1 - grp}))
        w_last.append(send(mine, wbuf.at[w_rows(3, grp, c)], wss.at[2, c], wrs.at[2, c], 0, 1))

    def w_close(c):
        w_side[c].wait_recv()
        w_last.append(
            send(
                wbuf.at[w_rows(2, 1 - grp, c)], wbuf.at[w_rows(3, 1 - grp, c)], wss.at[3, c],
                wrs.at[3, c], 0, 1,
            )
        )

    for c in range(EARLY):
        w_open(c)
    w_near = send(w_ref, w_at(1), wss.at[4, 0], wrs.at[4, 0], 0, 1)

    ii = lax.broadcasted_iota(jnp.int32, (rows, rows), 0)
    jj = lax.broadcasted_iota(jnp.int32, (rows, rows), 1)
    low = jnp.where(jj < ii, 1.0, 0.0).astype(bf)
    upp = jnp.where(ii < jj, 1.0, 0.0).astype(bf)

    def relative(first):
        return jnp.where(first < sp * epg, first + n_sp * epg, first) - sp * epg

    lane = lax.broadcasted_iota(jnp.int32, (rows, 128), 1)
    rel_r = relative(routes_t_ref[0:1, :])
    rel_r2 = relative(routes_t_ref[1:2, :])
    rel_c = jnp.sum(jnp.where(ii == jj, rel_r, 0), axis=1, keepdims=True)
    hot_c = jnp.where((rel_c >= lane * epg) & (rel_c < (lane + 1) * epg), 1.0, 0.0)
    rank_c = jnp.dot(low, hot_c.astype(bf), preferred_element_type=f32)
    lane_f = lane.astype(f32)
    slot_c = jnp.sum(hot_c * (lane_f * cap + rank_c), axis=1, keepdims=True)
    wide_c = jnp.sum(hot_c * (lane_f * 128 + rank_c), axis=1, keepdims=True)
    lane_s = lax.broadcasted_iota(jnp.int32, (rows, n_sp * cap), 1).astype(f32)
    pt_ref[...] = jnp.where(lane_s == slot_c, 1.0, 0.0).astype(bf)
    lane_w = lax.broadcasted_iota(jnp.int32, (rows, n_sp * 128), 1).astype(f32)
    pt_wide = jnp.where(lane_w == wide_c, 1.0, 0.0).astype(bf)

    sub = lax.broadcasted_iota(jnp.int32, (16, rows), 0)
    sub_f = sub.astype(f32)
    hot_r = jnp.where((rel_r >= sub * epg) & (rel_r < (sub + 1) * epg), 1.0, 0.0)
    rank_r = jnp.dot(hot_r.astype(bf), upp, preferred_element_type=f32)
    slot_r = jnp.sum(hot_r * (sub_f * cap + rank_r), axis=0, keepdims=True)
    group_r = jnp.sum(hot_r * sub_f, axis=0, keepdims=True)
    sub_s = lax.broadcasted_iota(jnp.int32, (cap, rows), 0).astype(f32)

    def chosen(d):
        return jnp.where(sub_s + float(d * cap) == slot_r, 1.0, 0.0).astype(bf)

    far = {}

    def send_rows(d):
        picked = jnp.dot(chosen(d), res_ref[...], preferred_element_type=f32).astype(bf)
        if d == 0:
            own_r[0] = picked
            return
        xs[d] = picked
        far[0, d] = send(xs.at[d], rres.at[d], zss.at[0, d], zrs.at[0, d], d, 0)

    own = {}

    def own_cast(kind, src, dst, via):
        buf = own_a if kind else own_r
        own[kind, dst] = send(
            buf.at[src], buf.at[dst], oss.at[kind, dst], ors.at[kind, dst], 0, via
        )

    send_rows(ORDER[1])
    send_rows(0)
    own_cast(0, 0, 1, 1)

    for j in range(q_ref.shape[1] // 128):
        cs = pl.ds(j * 128, 128)
        rq[:, cs] = turn(q_ref[:, cs].astype(f32)).astype(bf)

    first_r = rel_r.astype(f32) - epg * group_r
    second_r = rel_r2.astype(f32) - epg * group_r
    w_t = jnp.where(first_r == sub_f, rw_t_ref[0:1, :], 0.0) + jnp.where(
        second_r == sub_f, rw_t_ref[1:2, :], 0.0
    )
    hi = w_t.astype(bf)
    rest = w_t - hi.astype(f32)
    mid = rest.astype(bf)
    lo = (rest - mid.astype(f32)).astype(bf)
    placed = (
        jnp.dot(hi, pt_wide, preferred_element_type=f32)
        + jnp.dot(mid, pt_wide, preferred_element_type=f32)
        + jnp.dot(lo, pt_wide, preferred_element_type=f32)
    )
    for d in range(n_sp):
        meta[d] = placed[0:8, d * 128 : (d + 1) * 128]
    meta_rx[0, 0] = placed[0:8, 0:128]
    metas = {}
    for d in range(n_sp):
        for k in range(n_tp):
            if d or k:
                metas[d, k] = send(
                    meta.at[d], meta_rx.at[d, k], mss.at[d, k], mrs.at[d, k], d, k
                )

    n_heads = q_ref.shape[1] // HDIM
    tail.wait_recv()
    qi = lax.broadcasted_iota(jnp.int32, (WINDOW, 2 * WINDOW), 0)
    ki = lax.broadcasted_iota(jnp.int32, (WINDOW, 2 * WINDOW), 1)
    band = (ki > qi) & (ki <= qi + WINDOW)

    def attend(k):
        n = tp_at(k)
        start = pl.multiple_of(n * WINDOW, WINDOW)
        keys = kv[pl.ds(start, 2 * WINDOW), 0:HDIM]
        vals = kv[pl.ds(start, 2 * WINDOW), HDIM : 2 * HDIM]
        q = rq[pl.ds(start, WINDOW), :]
        first = jnp.where((sp == 0) & (n == 0), WINDOW, 0)
        seen = band & (ki >= first)
        outs = []
        for h in range(n_heads):
            sc = lax.dot_general(
                q[:, h * HDIM : (h + 1) * HDIM], keys, (((1,), (1,)), ((), ())),
                preferred_element_type=f32,
            ) * HDIM ** (-0.5)
            sc = jnp.where(seen, sc, -jnp.inf)
            sink = sink_ref[0:1, h : h + 1]
            top = jnp.maximum(jnp.max(sc, axis=1, keepdims=True), sink)
            e = jnp.exp(sc - top)
            den = jnp.sum(e, axis=1, keepdims=True) + jnp.exp(sink - top)
            pr = (e * (1.0 / den)).astype(bf)
            outs.append(jnp.dot(pr, vals, preferred_element_type=f32))
        heads_v[k] = jnp.concatenate(outs, axis=1).astype(bf)

    heads = {}

    def send_heads(k):
        heads[k] = send(heads_v.at[k], abuf.at[k], ass_.at[k], ars.at[k], 0, k)

    tile = width // 4

    def project(d):
        def step(i, _):
            cols = pl.ds(pl.multiple_of(i * tile, tile), tile)
            acc[:, cols] = jnp.dot(rat[d], wbuf[:, cols], preferred_element_type=f32)
            return 0

        lax.fori_loop(0, 4, step, 0)

    def pack_heads(k):
        block = abuf[k] if k else heads_v[0]
        cs = pl.ds(k * depth, depth)
        for d in ORDER:
            picked = jnp.dot(chosen(d), block, preferred_element_type=f32).astype(bf)
            if d:
                aps[d, :, cs] = picked
            else:
                own_a[0, :, cs] = picked

    def send_heads_far(d):
        far[1, d] = send(aps.at[d], rat.at[d], zss.at[1, d], zrs.at[1, d], d, 0)

    attend(2)
    send_heads(2)
    attend(3)
    send_heads(3)
    for c in range(EARLY, PIECES):
        w_open(c)
    own_cast(0, 0, 2, 2)
    w_cross(0)
    attend(1)
    send_heads(1)
    attend(0)
    w_cross(1)
    pack_heads(0)
    heads[1].wait_recv()
    pack_heads(1)
    w_close(0)
    heads[2].wait_recv()
    pack_heads(2)
    heads[3].wait_recv()
    pack_heads(3)
    send_heads_far(ORDER[1])
    own_cast(1, 0, 2, 2)
    own_cast(1, 0, 1, 1)
    send_rows(ORDER[2])
    send_heads_far(ORDER[2])
    send_rows(ORDER[3])
    send_heads_far(ORDER[3])
    local[0].wait()
    w_near.wait_recv()
    w_close(1)
    w_cross(2)
    w_cross(3)
    w_close(2)
    w_close(3)
    for c in w_last:
        c.wait_recv()

    def shift(kind, _):
        own[kind, 2].wait_recv()
        own_cast(kind, 2, 3, 1)

    def gather(_, __):
        for kind in range(2):
            own[kind, 1].wait_recv()
            own[kind, 3].wait_recv()

        def step(t, _):
            cols = pl.ds(pl.multiple_of(t * tile, tile), tile)
            left = [
                jnp.concatenate(
                    [own_a[k, :, (i ^ k) * depth : ((i ^ k) + 1) * depth] for i in range(n_tp)], axis=1
                )
                for k in range(n_tp)
            ]
            acc0[:, cols] = jnp.dot(
                jnp.concatenate(left, axis=0), wbuf[:, cols], preferred_element_type=f32
            )
            return 0

        lax.fori_loop(0, 4, step, 0)
        for k in range(n_tp):
            settle(0, k, own_r[k], acc0[k * cap : (k + 1) * cap])

    def settle(d, k, rest, total):
        stream = (rest.astype(f32) + total).astype(bf)
        if k == 0:
            stream_v[d] = stream
        stream_f = stream.astype(f32)
        scale = lax.rsqrt(jnp.mean(stream_f * stream_f, axis=-1, keepdims=True) + norm_eps)
        tok[d, k] = (stream_f * scale * gain_ref[...]).astype(bf)

    half_w = width // PARTS

    def part(h):
        return pl.ds(h * half_w, half_w)

    plane = {}

    def cast(src, dst, d, h, via):
        plane[dst, d, h] = send(
            tok.at[d, src, :, part(h)], tok.at[d, dst, :, part(h)], dss.at[dst, d, h],
            drs.at[dst, d, h], 0, via,
        )

    def spread(d, _):
        far[0, d].wait_recv()
        far[1, d].wait_recv()
        project(d)
        settle(d, 0, rres[d], acc[...])
        for h in range(PARTS):
            cast(0, 2, d, h, 2)
            cast(0, 1, d, h, 1)

    def relay(d, h):
        plane[2, d, h].wait_recv()
        cast(2, 3, d, h, 1)

    eye = lax.broadcasted_iota(jnp.int32, (cap, 128), 0) == lax.broadcasted_iota(
        jnp.int32, (cap, 128), 1
    )
    f_tile = ff // 2
    back = {}

    def serve(d, _):
        cols = []
        if d:
            for h in range(PARTS):
                plane[1, d, h].wait_recv()
                plane[3, d, h].wait_recv()
        for k in range(n_tp):
            if d or k:
                metas[d, k].wait_recv()
            row = meta_rx[d, k, pl.ds(tp, 1), :]
            cols.append(jnp.sum(jnp.where(eye, row, 0.0), axis=1, keepdims=True))
        weight = jnp.concatenate(cols, axis=0)

        def inner(i, _):
            cs = pl.ds(pl.multiple_of(i * f_tile, f_tile), f_tile)
            x = tok[d].reshape(n_tp * cap, width)
            g = jnp.dot(x, gate_v[:, cs], preferred_element_type=f32)
            u = jnp.dot(x, up_v[:, cs], preferred_element_type=f32)
            hid[:, cs] = (g / (1.0 + jnp.exp(-g)) * u * weight).astype(bf)
            return 0

        lax.fori_loop(0, 2, inner, 0)
        def outer(i, _):
            cs = pl.ds(pl.multiple_of(i * tile, tile), tile)
            o = jnp.dot(hid[...], down_v[:, cs], preferred_element_type=f32).astype(bf)
            y[d, :, :, cs] = o.reshape(n_tp, cap, tile)
            return 0

        per = 4 // PARTS
        for h in range(PARTS):
            lax.fori_loop(h * per, (h + 1) * per, outer, 0)
            for k, slot in ((3, 1), (1, 0)):
                back[k, d, h] = send(
                    y.at[d, k, :, part(h)], yr.at[d, slot, :, part(h)], rss.at[slot, d, h],
                    rrs.at[slot, d, h], 0, 1,
                )

    def pair(d, h):
        cs = part(h)
        back[3, d, h].wait_recv()
        sum2[d, :, cs] = (y[d, 2, :, cs].astype(f32) + yr[d, 1, :, cs].astype(f32)).astype(bf)
        back[2, d, h] = send(
            sum2.at[d, :, cs], xrec.at[d, :, cs], rss.at[2, d, h], rrs.at[2, d, h], 0, 2
        )
        back[1, d, h].wait_recv()
        sum0[d, :, cs] = y[d, 0, :, cs].astype(f32) + yr[d, 0, :, cs].astype(f32)

    home = {}

    def finish(d, h):
        cs = part(h)
        back[2, d, h].wait_recv()
        total = (stream_v[d, :, cs].astype(f32) + sum0[d, :, cs] + xrec[d, :, cs].astype(f32)).astype(bf)
        if d:
            zsend[d, :, cs] = total
            home[d, h] = send(
                zsend.at[d, :, cs], zrec.at[d, :, cs], rss.at[3, d, h], rrs.at[3, d, h],
                n_sp - d, 0,
            )
        else:
            zrec[0, :, cs] = total

    steps = (
        (shift, 0, 0),
        (spread, 2, 0),
        (shift, 1, 0),
        (gather, 0, 0),
        (spread, 1, 0),
        (relay, 2, 0),
        (relay, 2, 1),
        (serve, 2, 0),
        (pair, 2, 0),
        (pair, 2, 1),
        (serve, 0, 0),
        (spread, 3, 0),
        (relay, 1, 0),
        (relay, 1, 1),
        (serve, 1, 0),
        (finish, 2, 0),
        (finish, 2, 1),
        (pair, 1, 0),
        (pair, 1, 1),
        (relay, 3, 0),
        (relay, 3, 1),
        (serve, 3, 0),
        (finish, 1, 0),
        (finish, 1, 1),
        (pair, 3, 0),
        (pair, 3, 1),
        (pair, 0, 0),
        (finish, 3, 0),
        (pair, 0, 1),
        (finish, 3, 1),
        (finish, 0, 0),
        (finish, 0, 1),
    )
    for c in local[1:]:
        c.wait()
    for stage, d, h in steps:
        stage(d, h)
    def close(i, _):
        cs = pl.ds(pl.multiple_of(i * tile, tile), tile)
        rec = zrec[:, :, cs].reshape(n_sp * cap, tile)
        got = jnp.dot(pt_ref[...], rec, preferred_element_type=f32)
        out_ref[:, cs] = got.astype(bf)
        return 0

    for h in range(PARTS):
        for d in ORDER[1:]:
            home[d, h].wait_recv()
        lax.fori_loop(h * 4 // PARTS, (h + 1) * 4 // PARTS, close, 0)
    for c in sends:
        c.wait_send()


def whole_layer(
    query_rows, key_rows, value_rows, sink_logits, residual, out_weight, norm_gain, gate_weight, up_weight, down_weight, routes,
    route_weight,
):
    n_tp = lax.axis_size("tp")
    n_sp = lax.axis_size("sp")
    rows, width = residual.shape
    ff = gate_weight.shape[2]
    depth = out_weight.shape[0]
    cap = 2 * rows // n_sp
    toks = query_rows.shape[0]
    half_dim = HDIM // 2
    inverse = rope_base ** (-jnp.arange(half_dim, dtype=jnp.float32) / half_dim)
    bf = jnp.bfloat16
    f32 = jnp.float32
    dma = pltpu.SemaphoreType.DMA
    vm = pl.BlockSpec(memory_space=pltpu.VMEM)
    hbm = pl.BlockSpec(memory_space=pl.ANY)
    return pl.pallas_call(
        layer_kernel,
        out_shape=jax.ShapeDtypeStruct((rows, width), bf),
        in_specs=[vm] * 5 + [hbm, vm, vm, vm, vm, hbm, hbm, hbm],
        out_specs=vm,
        scratch_shapes=[
            pltpu.VMEM((n_tp * depth, width), bf),
            pltpu.VMEM((n_tp, rows, depth), bf),
            pltpu.VMEM((cap, width), f32),
            pltpu.VMEM((n_sp, cap, width), bf),
            pltpu.VMEM((n_sp, cap, width), bf),
            pltpu.VMEM((n_sp, cap, n_tp * depth), bf),
            pltpu.VMEM((n_sp, cap, n_tp * depth), bf),
            pltpu.VMEM((n_tp, cap, width), bf),
            pltpu.VMEM((n_tp, cap, n_tp * depth), bf),
            pltpu.VMEM((n_tp * cap, width), f32),
            pltpu.VMEM((n_sp, n_tp, cap, width), bf),
            pltpu.VMEM((width, ff), bf),
            pltpu.VMEM((width, ff), bf),
            pltpu.VMEM((ff, width), bf),
            pltpu.VMEM((n_tp * cap, ff), bf),
            pltpu.VMEM((n_sp, n_tp, cap, width), bf),
            pltpu.VMEM((n_sp, 2, cap, width), bf),
            pltpu.VMEM((n_sp, cap, width), f32),
            pltpu.VMEM((n_sp, cap, width), bf),
            pltpu.VMEM((n_sp, cap, width), bf),
            pltpu.VMEM((n_sp, cap, width), bf),
            pltpu.VMEM((n_sp, cap, width), bf),
            pltpu.VMEM((n_sp, 8, 128), f32),
            pltpu.VMEM((n_sp, n_tp, 8, 128), f32),
            pltpu.VMEM((rows, n_sp * cap), bf),
            pltpu.VMEM((n_sp, cap, width), bf),
            pltpu.VMEM((toks + WINDOW, 2 * HDIM), bf),
            pltpu.VMEM((toks, depth), bf),
            pltpu.VMEM((n_tp, rows, depth), bf),
            pltpu.VMEM((toks, 128), f32),
            pltpu.VMEM((toks, 128), f32),
            dma((4,)), dma((5, PIECES)), dma((5, PIECES)), dma, dma, dma((4,)), dma((4,)),
            dma((n_sp, n_tp)), dma((n_sp, n_tp)), dma((2, n_sp)), dma((2, n_sp)),
            dma((2, n_tp)), dma((2, n_tp)),
            dma((4, n_sp, PARTS)), dma((4, n_sp, PARTS)), dma((4, n_sp, PARTS)),
            dma((4, n_sp, PARTS)),
        ],
        compiler_params=pltpu.CompilerParams(
            collective_id=0, has_side_effects=True, vmem_limit_bytes=60000 * 1024
        ),
        name="routed_layer",
    )(
        query_rows, key_rows.T, value_rows.T, jnp.tile(inverse, 4)[None, :], sink_logits[None, :],
        out_weight,
        residual, norm_gain[None, :],
        routes.T, route_weight.T, gate_weight[0], up_weight[0], down_weight[0],
    )


def per_device(
    query_rows,
    key_rows,
    value_rows,
    sink_logits,
    residual,
    out_weight,
    norm_gain,
    gate_weight,
    up_weight,
    down_weight,
    routes,
    route_weight,
):
    tok_count = query_rows.shape[0]
    fits = (
        lax.axis_size("grp") == 2
        and lax.axis_size("sp") == GROUPS
        and lax.axis_size("tp") == 4
        and residual.shape[0] == WINDOW
        and key_rows.shape[1] == HDIM
        and query_rows.shape[1] % 128 == 0
    )
    if fits:
        return whole_layer(
            query_rows, key_rows, value_rows, sink_logits, residual, out_weight, norm_gain,
            gate_weight, up_weight, down_weight, routes, route_weight,
        )
    head_local = query_rows.shape[1] // HDIM
    group_local = key_rows.shape[1] // HDIM
    repeat = head_local // group_local
    first_pos = lax.axis_index("sp") * tok_count
    positions = first_pos + jnp.arange(tok_count, dtype=jnp.int32)
    rot_q = rotate(query_rows, positions, head_local)
    rot_k = rotate(key_rows, positions, group_local)
    tails = jnp.stack([rot_k[tok_count - WINDOW :], value_rows[tok_count - WINDOW :]])
    earlier = shifted(tails, "sp", 1)
    blocks = tok_count // WINDOW
    q_blocks = rot_q.reshape(blocks, WINDOW, group_local, repeat, HDIM)
    k_blocks = rot_k.reshape(blocks, WINDOW, group_local, HDIM)
    v_blocks = value_rows.reshape(blocks, WINDOW, group_local, HDIM)
    k_prev = jnp.concatenate(
        [earlier[0].reshape(1, WINDOW, group_local, HDIM), k_blocks[:-1]], axis=0
    )
    v_prev = jnp.concatenate(
        [earlier[1].reshape(1, WINDOW, group_local, HDIM), v_blocks[:-1]], axis=0
    )
    k_wide = jnp.concatenate([k_prev, k_blocks], axis=1)
    v_wide = jnp.concatenate([v_prev, v_blocks], axis=1)
    query_pos = jnp.arange(WINDOW) + WINDOW
    key_pos = jnp.arange(2 * WINDOW)
    distance = query_pos[:, None] - key_pos[None, :]
    in_band = (distance >= 0) & (distance < WINDOW)
    key_global = (
        first_pos + jnp.arange(blocks)[:, None, None] * WINDOW + key_pos[None, None, :] - WINDOW
    )
    allowed = in_band[None] & (key_global >= 0)
    scores = jnp.einsum(
        "nqgrd,nkgd->grnqk", q_blocks, k_wide, preferred_element_type=jnp.float32
    ) * HDIM ** (-0.5)
    scores = jnp.where(allowed[None, None], scores, -jnp.inf)
    sink_here = sink_logits.reshape(group_local, repeat)[:, :, None, None, None]
    largest = jnp.maximum(scores.max(axis=-1, keepdims=True), sink_here)
    exp_scores = jnp.exp(scores - largest)
    denominator = exp_scores.sum(axis=-1, keepdims=True) + jnp.exp(sink_here - largest)
    probs = (exp_scores / denominator).astype(jnp.bfloat16)
    attended = jnp.einsum("grnqk,nkgd->nqgrd", probs, v_wide, preferred_element_type=jnp.float32)
    attended = attended.astype(jnp.bfloat16).reshape(tok_count, head_local * HDIM)
    row_count = residual.shape[0]
    token_rows = lax.all_to_all(attended, "tp", split_axis=0, concat_axis=1, tiled=True)
    projected = jnp.dot(
        token_rows,
        lax.all_gather(out_weight, "tp", axis=0, tiled=True),
        preferred_element_type=jnp.float32,
    )
    stream_f = (residual.astype(jnp.float32) + projected).astype(jnp.bfloat16).astype(jnp.float32)
    normed = (
        stream_f
        * lax.rsqrt(jnp.mean(stream_f * stream_f, axis=-1, keepdims=True) + norm_eps)
        * norm_gain[None, :]
    ).astype(jnp.bfloat16)
    sp_count = lax.axis_size("sp")
    tp_count = lax.axis_size("tp")
    expert_count = sp_count * tp_count
    capacity = 4 * row_count // expert_count
    width = normed.shape[1]
    flat_expert = routes.reshape(-1)
    one_hot = (flat_expert[:, None] == jnp.arange(expert_count, dtype=jnp.int32)[None, :]).astype(
        jnp.int32
    )
    slot_rank = jnp.sum((jnp.cumsum(one_hot, axis=0) - one_hot) * one_hot, axis=1)
    slot_index = flat_expert * capacity + slot_rank
    token_of = jnp.arange(2 * row_count, dtype=jnp.int32) // 2
    outgoing = (
        jnp.zeros((expert_count * capacity, width), jnp.bfloat16)
        .at[slot_index]
        .set(normed[token_of])
    )
    outgoing = outgoing.reshape(expert_count, capacity, width)
    arrived = lax.all_to_all(outgoing, ("sp", "tp"), split_axis=0, concat_axis=0, tiled=True)
    flat_rows = arrived.reshape(-1, width)
    gate_out = jnp.dot(flat_rows, gate_weight[0], preferred_element_type=jnp.float32)
    up_out = jnp.dot(flat_rows, up_weight[0], preferred_element_type=jnp.float32)
    hidden = (jax.nn.silu(gate_out) * up_out).astype(jnp.bfloat16)
    produced = jnp.dot(hidden, down_weight[0], preferred_element_type=jnp.float32).astype(
        jnp.bfloat16
    )
    returned = lax.all_to_all(
        produced.reshape(arrived.shape), ("sp", "tp"), split_axis=0, concat_axis=0, tiled=True
    )
    gathered = returned.reshape(expert_count * capacity, width)[slot_index].astype(jnp.float32)
    weighted = gathered * route_weight.reshape(-1)[:, None]
    combined = weighted.reshape(row_count, 2, width).sum(axis=1)
    return (stream_f + combined).astype(jnp.bfloat16)


def solution(mesh):
    in_specs = (
        P(("grp", "sp"), "tp"),
        P(("grp", "sp"), "tp"),
        P(("grp", "sp"), "tp"),
        P("tp"),
        P(("grp", "sp", "tp"), None),
        P("tp", None),
        P(),
        P(("sp", "tp"), None, None),
        P(("sp", "tp"), None, None),
        P(("sp", "tp"), None, None),
        P(("grp", "sp", "tp"), None),
        P(("grp", "sp", "tp"), None),
    )
    out_specs = P(("grp", "sp", "tp"), None)
    return jax.shard_map(
        per_device, mesh=mesh, in_specs=in_specs, out_specs=out_specs, check_vma=False
    )
```

```python
import functools

import jax
import jax.numpy as jnp
from jax import lax
from jax.experimental import pallas as pl
from jax.experimental.pallas import tpu as pltpu
from jax.sharding import PartitionSpec as P

HDIM = 64
WINDOW = 128
GROUPS = 4
MESH = pl.DeviceIdType.MESH


rope_base = 10000.0
norm_eps = 1e-06


def shifted(block, axis, distance):
    devices = range(lax.axis_size(axis))
    route = [(i - distance, i) for i in devices if i - distance in devices]
    return lax.ppermute(block, axis, route)


def rotate(rows, positions, heads):
    half_dim = HDIM // 2
    values = rows.astype(jnp.float32).reshape(rows.shape[0], heads, HDIM)
    inverse = rope_base ** (-jnp.arange(half_dim, dtype=jnp.float32) / half_dim)
    angles = positions.astype(jnp.float32)[:, None] * inverse[None, :]
    cosines = jnp.cos(angles)[:, None, :]
    sines = jnp.sin(angles)[:, None, :]
    lower = values[..., :half_dim]
    upper = values[..., half_dim:]
    turned = jnp.concatenate(
        [lower * cosines - upper * sines, upper * cosines + lower * sines], axis=-1
    )
    return turned.reshape(rows.shape[0], heads * HDIM).astype(jnp.bfloat16)


ORDER = (0, 1, 2, 3)
PIECES = 8
EARLY = 4
PARTS = 2


def layer_kernel(
    q_ref, k_ref, v_ref, inv_ref, sink_ref, w_ref, res_ref, gain_ref, routes_t_ref, rw_t_ref, gate_ref, up_ref,
    down_ref, out_ref,
    wbuf, abuf, acc, xs, rres, aps, rat, own_r, own_a, acc0, tok, gate_v, up_v, down_v, hid, y, yr, sum0, sum2, xrec, zsend, zrec,
    meta, meta_rx, pt_ref, stream_v, kv, rq, heads_v, cos_ref, sin_ref,
    lsem, wss, wrs, kss, krs, ass_, ars, mss, mrs, zss, zrs, oss, ors, dss, drs, rss, rrs,
):
    grp = lax.axis_index("grp")
    sp = lax.axis_index("sp")
    tp = lax.axis_index("tp")
    n_sp = GROUPS
    n_tp = 4
    rows = res_ref.shape[0]
    width = res_ref.shape[1]
    cap = xs.shape[1]
    epg = n_tp
    ff = gate_ref.shape[1]

    def sp_at(d):
        return lax.bitwise_xor(sp, d)

    near = tp + 1 - 2 * lax.rem(tp, 2)

    def tp_at(k):
        base = near if k % 2 else tp
        return lax.rem(base + 2, n_tp) if k >= 2 else base

    depth = w_ref.shape[0]

    def w_at(k):
        return wbuf.at[pl.ds(k * depth, depth)]

    local = [
        pltpu.make_async_copy(w_ref, w_at(0), lsem.at[0]),
        pltpu.make_async_copy(gate_ref, gate_v, lsem.at[1]),
        pltpu.make_async_copy(up_ref, up_v, lsem.at[2]),
        pltpu.make_async_copy(down_ref, down_v, lsem.at[3]),
    ]
    for c in local:
        c.start()

    barrier = pltpu.get_barrier_semaphore()
    for d in range(n_sp):
        for k in range(n_tp):
            if d or k:
                pl.semaphore_signal(
                    barrier, inc=1, device_id={"sp": sp_at(d), "tp": tp_at(k)},
                    device_id_type=MESH,
                )
    pl.semaphore_signal(
        barrier, inc=1, device_id={"grp": 1 - grp}, device_id_type=MESH
    )

    f32 = jnp.float32
    bf = jnp.bfloat16
    toks = q_ref.shape[0]
    half_dim = HDIM // 2
    lane_t = lax.broadcasted_iota(jnp.int32, (toks, 128), 1)
    lower = lax.rem(lane_t, HDIM) < half_dim

    def turn(x):
        other = jnp.where(
            lower, pltpu.roll(x, 128 - half_dim, 1), pltpu.roll(x, half_dim, 1)
        )
        return x * cos_ref[...] + other * sin_ref[...]

    pos = lax.broadcasted_iota(jnp.int32, (toks, 128), 0) + sp * toks
    angle = pos.astype(f32) * inv_ref[...]
    cos_ref[...] = jnp.cos(angle)
    sines = jnp.sin(angle)
    sin_ref[...] = jnp.where(lower, -sines, sines)
    both = jnp.concatenate([k_ref[...], v_ref[...]], axis=0).T
    turned = turn(both.astype(f32)).astype(bf)
    kv[WINDOW:, :] = jnp.where(lane_t < HDIM, turned, both)
    pl.semaphore_wait(barrier, n_sp * n_tp)

    sends = []

    def plan(src, dst, ssem, rsem, where):
        c = pltpu.make_async_remote_copy(
            src_ref=src, dst_ref=dst, send_sem=ssem, recv_sem=rsem,
            device_id=where, device_id_type=MESH,
        )
        sends.append(c)
        return c

    def post(src, dst, ssem, rsem, where):
        c = plan(src, dst, ssem, rsem, where)
        c.start()
        return c

    def send(src, dst, ssem, rsem, d, k):
        return post(src, dst, ssem, rsem, {"sp": sp_at(d), "tp": tp_at(k)})

    tail = post(
        kv.at[pl.ds(toks, WINDOW)], kv.at[pl.ds(0, WINDOW)], kss, krs,
        {"sp": lax.rem(sp + 1, n_sp)},
    )
    chunk = depth // (2 * PIECES)

    def w_rows(k, half, c):
        return pl.ds(pl.multiple_of(k * depth + half * (depth // 2) + c * chunk, chunk), chunk)

    w_far = []

    def w_open(c):
        w_far.append(
            send(
                w_ref.at[w_rows(0, grp, c)], wbuf.at[w_rows(2, grp, c)], wss.at[0, c], wrs.at[0, c], 0, 2
            )
        )

    w_side, w_last = [], []

    def w_cross(c):
        w_far[c].wait_recv()
        mine = wbuf.at[w_rows(2, grp, c)]
        w_side.append(post(mine, mine, wss.at[1, c], wrs.at[1, c], {"grp": 1 - grp}))
        w_last.append(send(mine, wbuf.at[w_rows(3, grp, c)], wss.at[2, c], wrs.at[2, c], 0, 1))

    def w_close(c):
        w_side[c].wait_recv()
        w_last.append(
            send(
                wbuf.at[w_rows(2, 1 - grp, c)], wbuf.at[w_rows(3, 1 - grp, c)], wss.at[3, c],
                wrs.at[3, c], 0, 1,
            )
        )

    for c in range(EARLY):
        w_open(c)
    w_near = send(w_ref, w_at(1), wss.at[4, 0], wrs.at[4, 0], 0, 1)

    ii = lax.broadcasted_iota(jnp.int32, (rows, rows), 0)
    jj = lax.broadcasted_iota(jnp.int32, (rows, rows), 1)
    low = jnp.where(jj < ii, 1.0, 0.0).astype(bf)
    upp = jnp.where(ii < jj, 1.0, 0.0).astype(bf)

    def relative(first):
        return lax.bitwise_xor(first, jnp.broadcast_to(sp * epg, first.shape))

    lane = lax.broadcasted_iota(jnp.int32, (rows, 128), 1)
    rel_r = relative(routes_t_ref[0:1, :])
    rel_r2 = relative(routes_t_ref[1:2, :])
    rel_c = jnp.sum(jnp.where(ii == jj, rel_r, 0), axis=1, keepdims=True)
    hot_c = jnp.where((rel_c >= lane * epg) & (rel_c < (lane + 1) * epg), 1.0, 0.0)
    rank_c = jnp.dot(low, hot_c.astype(bf), preferred_element_type=f32)
    lane_f = lane.astype(f32)
    slot_c = jnp.sum(hot_c * (lane_f * cap + rank_c), axis=1, keepdims=True)
    wide_c = jnp.sum(hot_c * (lane_f * 128 + rank_c), axis=1, keepdims=True)
    lane_s = lax.broadcasted_iota(jnp.int32, (rows, n_sp * cap), 1).astype(f32)
    pt_ref[...] = jnp.where(lane_s == slot_c, 1.0, 0.0).astype(bf)
    lane_w = lax.broadcasted_iota(jnp.int32, (rows, n_sp * 128), 1).astype(f32)
    pt_wide = jnp.where(lane_w == wide_c, 1.0, 0.0).astype(bf)

    sub = lax.broadcasted_iota(jnp.int32, (16, rows), 0)
    sub_f = sub.astype(f32)
    hot_r = jnp.where((rel_r >= sub * epg) & (rel_r < (sub + 1) * epg), 1.0, 0.0)
    rank_r = jnp.dot(hot_r.astype(bf), upp, preferred_element_type=f32)
    slot_r = jnp.sum(hot_r * (sub_f * cap + rank_r), axis=0, keepdims=True)
    group_r = jnp.sum(hot_r * sub_f, axis=0, keepdims=True)
    sub_s = lax.broadcasted_iota(jnp.int32, (cap, rows), 0).astype(f32)

    def chosen(d):
        return jnp.where(sub_s + float(d * cap) == slot_r, 1.0, 0.0).astype(bf)

    far = {}

    def send_rows(d):
        picked = jnp.dot(chosen(d), res_ref[...], preferred_element_type=f32).astype(bf)
        if d == 0:
            own_r[0] = picked
            return
        xs[d] = picked
        far[0, d] = plan(
            xs.at[d], rres.at[d], zss.at[0, d], zrs.at[0, d], {"sp": sp_at(d), "tp": tp_at(0)}
        )
        if d < n_sp - 1:
            far[0, d].start()

    own = {}

    def own_cast(kind, src, dst, via):
        buf = own_a if kind else own_r
        own[kind, dst] = send(
            buf.at[src], buf.at[dst], oss.at[kind, dst], ors.at[kind, dst], 0, via
        )

    send_rows(1)
    send_rows(2)
    send_rows(0)
    own_cast(0, 0, 1, 1)

    for j in range(q_ref.shape[1] // 128):
        cs = pl.ds(j * 128, 128)
        rq[:, cs] = turn(q_ref[:, cs].astype(f32)).astype(bf)

    first_r = rel_r.astype(f32) - epg * group_r
    second_r = rel_r2.astype(f32) - epg * group_r
    w_t = jnp.where(first_r == sub_f, rw_t_ref[0:1, :], 0.0) + jnp.where(
        second_r == sub_f, rw_t_ref[1:2, :], 0.0
    )
    hi = w_t.astype(bf)
    rest = w_t - hi.astype(f32)
    mid = rest.astype(bf)
    lo = (rest - mid.astype(f32)).astype(bf)
    placed = (
        jnp.dot(hi, pt_wide, preferred_element_type=f32)
        + jnp.dot(mid, pt_wide, preferred_element_type=f32)
        + jnp.dot(lo, pt_wide, preferred_element_type=f32)
    )
    for d in range(n_sp):
        meta[d] = placed[0:8, d * 128 : (d + 1) * 128]
    meta_rx[0, 0] = placed[0:8, 0:128]
    metas = {}
    for d in range(n_sp):
        for k in range(n_tp):
            if d or k:
                metas[d, k] = send(
                    meta.at[d], meta_rx.at[d, k], mss.at[d, k], mrs.at[d, k], d, k
                )

    n_heads = q_ref.shape[1] // HDIM
    tail.wait_recv()
    qi = lax.broadcasted_iota(jnp.int32, (WINDOW, 2 * WINDOW), 0)
    ki = lax.broadcasted_iota(jnp.int32, (WINDOW, 2 * WINDOW), 1)
    band = (ki > qi) & (ki <= qi + WINDOW)

    def attend(k):
        n = tp_at(k)
        start = pl.multiple_of(n * WINDOW, WINDOW)
        keys = kv[pl.ds(start, 2 * WINDOW), 0:HDIM]
        vals = kv[pl.ds(start, 2 * WINDOW), HDIM : 2 * HDIM]
        q = rq[pl.ds(start, WINDOW), :]
        first = jnp.where((sp == 0) & (n == 0), WINDOW, 0)
        seen = band & (ki >= first)
        outs = []
        for h in range(n_heads):
            sc = lax.dot_general(
                q[:, h * HDIM : (h + 1) * HDIM], keys, (((1,), (1,)), ((), ())),
                preferred_element_type=f32,
            ) * HDIM ** (-0.5)
            sc = jnp.where(seen, sc, -jnp.inf)
            sink = sink_ref[0:1, h : h + 1]
            top = jnp.maximum(jnp.max(sc, axis=1, keepdims=True), sink)
            e = jnp.exp(sc - top)
            den = jnp.sum(e, axis=1, keepdims=True) + jnp.exp(sink - top)
            pr = (e * (1.0 / den)).astype(bf)
            outs.append(jnp.dot(pr, vals, preferred_element_type=f32))
        heads_v[k] = jnp.concatenate(outs, axis=1).astype(bf)

    heads = {}

    def send_heads(k):
        heads[k] = send(heads_v.at[k], abuf.at[k], ass_.at[k], ars.at[k], 0, k)

    tile = width // 4

    def project(d):
        def step(i, _):
            cols = pl.ds(pl.multiple_of(i * tile, tile), tile)
            acc[:, cols] = jnp.dot(rat[d], wbuf[:, cols], preferred_element_type=f32)
            return 0

        lax.fori_loop(0, 4, step, 0)

    def pack_heads(k):
        block = abuf[k] if k else heads_v[0]
        cs = pl.ds(k * depth, depth)
        for d in ORDER:
            picked = jnp.dot(chosen(d), block, preferred_element_type=f32).astype(bf)
            if d:
                aps[d, :, cs] = picked
            else:
                own_a[0, :, cs] = picked

    def send_heads_far(d):
        far[1, d] = plan(
            aps.at[d], rat.at[d], zss.at[1, d], zrs.at[1, d], {"sp": sp_at(d), "tp": tp_at(0)}
        )
        if d < n_sp - 1:
            far[1, d].start()

    attend(2)
    send_heads(2)
    w_cross(0)
    attend(3)
    send_heads(3)
    for c in range(EARLY, PIECES):
        w_open(c)
    own_cast(0, 0, 2, 2)
    w_cross(1)
    attend(1)
    send_heads(1)
    w_cross(2)
    w_close(0)
    attend(0)
    w_cross(3)
    w_close(1)
    pack_heads(0)
    heads[1].wait_recv()
    pack_heads(1)
    w_close(2)
    heads[2].wait_recv()
    pack_heads(2)
    heads[3].wait_recv()
    pack_heads(3)
    send_heads_far(1)
    send_heads_far(2)
    own_cast(1, 0, 1, 1)
    own_cast(1, 0, 2, 2)
    send_rows(3)
    send_heads_far(3)
    inner = (sp == 1) | (sp == 2)

    def launch_last():
        far[0, 3].start()
        far[1, 3].start()

    local[0].wait()
    w_near.wait_recv()
    w_close(3)
    w_cross(4)
    w_cross(5)
    w_cross(6)
    w_close(4)
    pl.when(inner)(launch_last)
    w_cross(7)
    w_close(5)
    w_close(6)
    w_close(7)
    for c in w_last:
        c.wait_recv()

    def cross(*_):
        own_cast(1, 0, 2, 2)

    def rush(*_):
        pl.when(jnp.logical_not(inner))(launch_last)

    def shift(kind, _):
        own[kind, 2].wait_recv()
        own_cast(kind, 2, 3, 1)

    def gather(_, __):
        for kind in range(2):
            own[kind, 1].wait_recv()
            own[kind, 3].wait_recv()

        def step(t, _):
            cols = pl.ds(pl.multiple_of(t * tile, tile), tile)
            left = [
                jnp.concatenate(
                    [own_a[k, :, (i ^ k) * depth : ((i ^ k) + 1) * depth] for i in range(n_tp)], axis=1
                )
                for k in range(n_tp)
            ]
            acc0[:, cols] = jnp.dot(
                jnp.concatenate(left, axis=0), wbuf[:, cols], preferred_element_type=f32
            )
            return 0

        lax.fori_loop(0, 4, step, 0)
        for k in range(n_tp):
            settle(0, k, own_r[k], acc0[k * cap : (k + 1) * cap])

    def settle(d, k, rest, total):
        stream = (rest.astype(f32) + total).astype(bf)
        if k == 0:
            stream_v[d] = stream
        stream_f = stream.astype(f32)
        scale = lax.rsqrt(jnp.mean(stream_f * stream_f, axis=-1, keepdims=True) + norm_eps)
        tok[d, k] = (stream_f * scale * gain_ref[...]).astype(bf)

    half_w = width // PARTS

    def part(h):
        return pl.ds(h * half_w, half_w)

    plane = {}

    def cast(src, dst, d, h, via):
        plane[dst, d, h] = send(
            tok.at[d, src, :, part(h)], tok.at[d, dst, :, part(h)], dss.at[dst, d, h],
            drs.at[dst, d, h], 0, via,
        )

    def spread(d, _):
        far[0, d].wait_recv()
        far[1, d].wait_recv()
        project(d)
        settle(d, 0, rres[d], acc[...])
        for h in range(PARTS):
            cast(0, 2, d, h, 2)
            cast(0, 1, d, h, 1)

    def relay(d, h):
        plane[2, d, h].wait_recv()
        cast(2, 3, d, h, 1)

    eye = lax.broadcasted_iota(jnp.int32, (cap, 128), 0) == lax.broadcasted_iota(
        jnp.int32, (cap, 128), 1
    )
    f_tile = ff // 2
    back = {}

    def serve(d, _):
        cols = []
        if d:
            for h in range(PARTS):
                plane[1, d, h].wait_recv()
                plane[3, d, h].wait_recv()
        for k in range(n_tp):
            if d or k:
                metas[d, k].wait_recv()
            row = meta_rx[d, k, pl.ds(tp, 1), :]
            cols.append(jnp.sum(jnp.where(eye, row, 0.0), axis=1, keepdims=True))
        weight = jnp.concatenate(cols, axis=0)

        def inner(i, _):
            cs = pl.ds(pl.multiple_of(i * f_tile, f_tile), f_tile)
            x = tok[d].reshape(n_tp * cap, width)
            g = jnp.dot(x, gate_v[:, cs], preferred_element_type=f32)
            u = jnp.dot(x, up_v[:, cs], preferred_element_type=f32)
            hid[:, cs] = (g / (1.0 + jnp.exp(-g)) * u * weight).astype(bf)
            return 0

        lax.fori_loop(0, 2, inner, 0)
        def outer(i, _):
            cs = pl.ds(pl.multiple_of(i * tile, tile), tile)
            o = jnp.dot(hid[...], down_v[:, cs], preferred_element_type=f32).astype(bf)
            y[d, :, :, cs] = o.reshape(n_tp, cap, tile)
            return 0

        per = 4 // PARTS
        for h in range(PARTS):
            lax.fori_loop(h * per, (h + 1) * per, outer, 0)
            for k, slot in ((3, 1), (1, 0)):
                back[k, d, h] = send(
                    y.at[d, k, :, part(h)], yr.at[d, slot, :, part(h)], rss.at[slot, d, h],
                    rrs.at[slot, d, h], 0, 1,
                )

    def pair(d, h):
        cs = part(h)
        back[3, d, h].wait_recv()
        sum2[d, :, cs] = (y[d, 2, :, cs].astype(f32) + yr[d, 1, :, cs].astype(f32)).astype(bf)
        back[2, d, h] = send(
            sum2.at[d, :, cs], xrec.at[d, :, cs], rss.at[2, d, h], rrs.at[2, d, h], 0, 2
        )
        back[1, d, h].wait_recv()
        sum0[d, :, cs] = y[d, 0, :, cs].astype(f32) + yr[d, 0, :, cs].astype(f32)

    home = {}

    def finish(d, h):
        cs = part(h)
        back[2, d, h].wait_recv()
        total = (stream_v[d, :, cs].astype(f32) + sum0[d, :, cs] + xrec[d, :, cs].astype(f32)).astype(bf)
        if d:
            zsend[d, :, cs] = total
            home[d, h] = send(
                zsend.at[d, :, cs], zrec.at[d, :, cs], rss.at[3, d, h], rrs.at[3, d, h],
                d, 0,
            )
        else:
            zrec[0, :, cs] = total

    steps = (
        (spread, 2, 0),
        (rush, 0, 0),
        (spread, 1, 0),
        (shift, 0, 0),
        (shift, 1, 0),
        (gather, 0, 0),
        (relay, 2, 0),
        (relay, 2, 1),
        (serve, 2, 0),
        (pair, 2, 0),
        (pair, 2, 1),
        (relay, 1, 0),
        (relay, 1, 1),
        (spread, 3, 0),
        (serve, 1, 0),
        (pair, 1, 0),
        (pair, 1, 1),
        (finish, 2, 0),
        (serve, 0, 0),
        (finish, 2, 1),
        (relay, 3, 0),
        (relay, 3, 1),
        (serve, 3, 0),
        (pair, 3, 0),
        (finish, 1, 0),
        (pair, 3, 1),
        (finish, 1, 1),
        (pair, 0, 0),
        (finish, 3, 0),
        (pair, 0, 1),
        (finish, 3, 1),
        (finish, 0, 0),
        (finish, 0, 1),
    )
    for c in local[1:]:
        c.wait()
    for stage, d, h in steps:
        stage(d, h)
    def close(i, _):
        cs = pl.ds(pl.multiple_of(i * tile, tile), tile)
        rec = zrec[:, :, cs].reshape(n_sp * cap, tile)
        got = jnp.dot(pt_ref[...], rec, preferred_element_type=f32)
        out_ref[:, cs] = got.astype(bf)
        return 0

    for h in range(PARTS):
        for d in ORDER[1:]:
            home[d, h].wait_recv()
        lax.fori_loop(h * 4 // PARTS, (h + 1) * 4 // PARTS, close, 0)
    for c in sends:
        c.wait_send()


def whole_layer(
    query_rows, key_rows, value_rows, sink_logits, residual, out_weight, norm_gain, gate_weight, up_weight, down_weight, routes,
    route_weight,
):
    n_tp = lax.axis_size("tp")
    n_sp = lax.axis_size("sp")
    rows, width = residual.shape
    ff = gate_weight.shape[2]
    depth = out_weight.shape[0]
    cap = 2 * rows // n_sp
    toks = query_rows.shape[0]
    half_dim = HDIM // 2
    inverse = rope_base ** (-jnp.arange(half_dim, dtype=jnp.float32) / half_dim)
    bf = jnp.bfloat16
    f32 = jnp.float32
    dma = pltpu.SemaphoreType.DMA
    vm = pl.BlockSpec(memory_space=pltpu.VMEM)
    hbm = pl.BlockSpec(memory_space=pl.ANY)
    return pl.pallas_call(
        layer_kernel,
        out_shape=jax.ShapeDtypeStruct((rows, width), bf),
        in_specs=[vm] * 5 + [hbm, vm, vm, vm, vm, hbm, hbm, hbm],
        out_specs=vm,
        scratch_shapes=[
            pltpu.VMEM((n_tp * depth, width), bf),
            pltpu.VMEM((n_tp, rows, depth), bf),
            pltpu.VMEM((cap, width), f32),
            pltpu.VMEM((n_sp, cap, width), bf),
            pltpu.VMEM((n_sp, cap, width), bf),
            pltpu.VMEM((n_sp, cap, n_tp * depth), bf),
            pltpu.VMEM((n_sp, cap, n_tp * depth), bf),
            pltpu.VMEM((n_tp, cap, width), bf),
            pltpu.VMEM((n_tp, cap, n_tp * depth), bf),
            pltpu.VMEM((n_tp * cap, width), f32),
            pltpu.VMEM((n_sp, n_tp, cap, width), bf),
            pltpu.VMEM((width, ff), bf),
            pltpu.VMEM((width, ff), bf),
            pltpu.VMEM((ff, width), bf),
            pltpu.VMEM((n_tp * cap, ff), bf),
            pltpu.VMEM((n_sp, n_tp, cap, width), bf),
            pltpu.VMEM((n_sp, 2, cap, width), bf),
            pltpu.VMEM((n_sp, cap, width), f32),
            pltpu.VMEM((n_sp, cap, width), bf),
            pltpu.VMEM((n_sp, cap, width), bf),
            pltpu.VMEM((n_sp, cap, width), bf),
            pltpu.VMEM((n_sp, cap, width), bf),
            pltpu.VMEM((n_sp, 8, 128), f32),
            pltpu.VMEM((n_sp, n_tp, 8, 128), f32),
            pltpu.VMEM((rows, n_sp * cap), bf),
            pltpu.VMEM((n_sp, cap, width), bf),
            pltpu.VMEM((toks + WINDOW, 2 * HDIM), bf),
            pltpu.VMEM((toks, depth), bf),
            pltpu.VMEM((n_tp, rows, depth), bf),
            pltpu.VMEM((toks, 128), f32),
            pltpu.VMEM((toks, 128), f32),
            dma((4,)), dma((5, PIECES)), dma((5, PIECES)), dma, dma, dma((4,)), dma((4,)),
            dma((n_sp, n_tp)), dma((n_sp, n_tp)), dma((2, n_sp)), dma((2, n_sp)),
            dma((2, n_tp)), dma((2, n_tp)),
            dma((4, n_sp, PARTS)), dma((4, n_sp, PARTS)), dma((4, n_sp, PARTS)),
            dma((4, n_sp, PARTS)),
        ],
        compiler_params=pltpu.CompilerParams(
            collective_id=0, has_side_effects=True, vmem_limit_bytes=60000 * 1024
        ),
        name="routed_layer",
    )(
        query_rows, key_rows.T, value_rows.T, jnp.tile(inverse, 4)[None, :], sink_logits[None, :],
        out_weight,
        residual, norm_gain[None, :],
        routes.T, route_weight.T, gate_weight[0], up_weight[0], down_weight[0],
    )


def per_device(
    query_rows,
    key_rows,
    value_rows,
    sink_logits,
    residual,
    out_weight,
    norm_gain,
    gate_weight,
    up_weight,
    down_weight,
    routes,
    route_weight,
):
    tok_count = query_rows.shape[0]
    fits = (
        lax.axis_size("grp") == 2
        and lax.axis_size("sp") == GROUPS
        and lax.axis_size("tp") == 4
        and residual.shape[0] == WINDOW
        and key_rows.shape[1] == HDIM
        and query_rows.shape[1] % 128 == 0
    )
    if fits:
        return whole_layer(
            query_rows, key_rows, value_rows, sink_logits, residual, out_weight, norm_gain,
            gate_weight, up_weight, down_weight, routes, route_weight,
        )
    head_local = query_rows.shape[1] // HDIM
    group_local = key_rows.shape[1] // HDIM
    repeat = head_local // group_local
    first_pos = lax.axis_index("sp") * tok_count
    positions = first_pos + jnp.arange(tok_count, dtype=jnp.int32)
    rot_q = rotate(query_rows, positions, head_local)
    rot_k = rotate(key_rows, positions, group_local)
    tails = jnp.stack([rot_k[tok_count - WINDOW :], value_rows[tok_count - WINDOW :]])
    earlier = shifted(tails, "sp", 1)
    blocks = tok_count // WINDOW
    q_blocks = rot_q.reshape(blocks, WINDOW, group_local, repeat, HDIM)
    k_blocks = rot_k.reshape(blocks, WINDOW, group_local, HDIM)
    v_blocks = value_rows.reshape(blocks, WINDOW, group_local, HDIM)
    k_prev = jnp.concatenate(
        [earlier[0].reshape(1, WINDOW, group_local, HDIM), k_blocks[:-1]], axis=0
    )
    v_prev = jnp.concatenate(
        [earlier[1].reshape(1, WINDOW, group_local, HDIM), v_blocks[:-1]], axis=0
    )
    k_wide = jnp.concatenate([k_prev, k_blocks], axis=1)
    v_wide = jnp.concatenate([v_prev, v_blocks], axis=1)
    query_pos = jnp.arange(WINDOW) + WINDOW
    key_pos = jnp.arange(2 * WINDOW)
    distance = query_pos[:, None] - key_pos[None, :]
    in_band = (distance >= 0) & (distance < WINDOW)
    key_global = (
        first_pos + jnp.arange(blocks)[:, None, None] * WINDOW + key_pos[None, None, :] - WINDOW
    )
    allowed = in_band[None] & (key_global >= 0)
    scores = jnp.einsum(
        "nqgrd,nkgd->grnqk", q_blocks, k_wide, preferred_element_type=jnp.float32
    ) * HDIM ** (-0.5)
    scores = jnp.where(allowed[None, None], scores, -jnp.inf)
    sink_here = sink_logits.reshape(group_local, repeat)[:, :, None, None, None]
    largest = jnp.maximum(scores.max(axis=-1, keepdims=True), sink_here)
    exp_scores = jnp.exp(scores - largest)
    denominator = exp_scores.sum(axis=-1, keepdims=True) + jnp.exp(sink_here - largest)
    probs = (exp_scores / denominator).astype(jnp.bfloat16)
    attended = jnp.einsum("grnqk,nkgd->nqgrd", probs, v_wide, preferred_element_type=jnp.float32)
    attended = attended.astype(jnp.bfloat16).reshape(tok_count, head_local * HDIM)
    row_count = residual.shape[0]
    token_rows = lax.all_to_all(attended, "tp", split_axis=0, concat_axis=1, tiled=True)
    projected = jnp.dot(
        token_rows,
        lax.all_gather(out_weight, "tp", axis=0, tiled=True),
        preferred_element_type=jnp.float32,
    )
    stream_f = (residual.astype(jnp.float32) + projected).astype(jnp.bfloat16).astype(jnp.float32)
    normed = (
        stream_f
        * lax.rsqrt(jnp.mean(stream_f * stream_f, axis=-1, keepdims=True) + norm_eps)
        * norm_gain[None, :]
    ).astype(jnp.bfloat16)
    sp_count = lax.axis_size("sp")
    tp_count = lax.axis_size("tp")
    expert_count = sp_count * tp_count
    capacity = 4 * row_count // expert_count
    width = normed.shape[1]
    flat_expert = routes.reshape(-1)
    one_hot = (flat_expert[:, None] == jnp.arange(expert_count, dtype=jnp.int32)[None, :]).astype(
        jnp.int32
    )
    slot_rank = jnp.sum((jnp.cumsum(one_hot, axis=0) - one_hot) * one_hot, axis=1)
    slot_index = flat_expert * capacity + slot_rank
    token_of = jnp.arange(2 * row_count, dtype=jnp.int32) // 2
    outgoing = (
        jnp.zeros((expert_count * capacity, width), jnp.bfloat16)
        .at[slot_index]
        .set(normed[token_of])
    )
    outgoing = outgoing.reshape(expert_count, capacity, width)
    arrived = lax.all_to_all(outgoing, ("sp", "tp"), split_axis=0, concat_axis=0, tiled=True)
    flat_rows = arrived.reshape(-1, width)
    gate_out = jnp.dot(flat_rows, gate_weight[0], preferred_element_type=jnp.float32)
    up_out = jnp.dot(flat_rows, up_weight[0], preferred_element_type=jnp.float32)
    hidden = (jax.nn.silu(gate_out) * up_out).astype(jnp.bfloat16)
    produced = jnp.dot(hidden, down_weight[0], preferred_element_type=jnp.float32).astype(
        jnp.bfloat16
    )
    returned = lax.all_to_all(
        produced.reshape(arrived.shape), ("sp", "tp"), split_axis=0, concat_axis=0, tiled=True
    )
    gathered = returned.reshape(expert_count * capacity, width)[slot_index].astype(jnp.float32)
    weighted = gathered * route_weight.reshape(-1)[:, None]
    combined = weighted.reshape(row_count, 2, width).sum(axis=1)
    return (stream_f + combined).astype(jnp.bfloat16)


def solution(mesh):
    in_specs = (
        P(("grp", "sp"), "tp"),
        P(("grp", "sp"), "tp"),
        P(("grp", "sp"), "tp"),
        P("tp"),
        P(("grp", "sp", "tp"), None),
        P("tp", None),
        P(),
        P(("sp", "tp"), None, None),
        P(("sp", "tp"), None, None),
        P(("sp", "tp"), None, None),
        P(("grp", "sp", "tp"), None),
        P(("grp", "sp", "tp"), None),
    )
    out_specs = P(("grp", "sp", "tp"), None)
    return jax.shard_map(
        per_device, mesh=mesh, in_specs=in_specs, out_specs=out_specs, check_vma=False
    )
```

```python
import functools

import jax
import jax.numpy as jnp
import numpy as np
from jax import lax
from jax.experimental import pallas as pl
from jax.experimental.pallas import tpu as pltpu
from jax.sharding import PartitionSpec as P

HDIM = 64
WINDOW = 128
GROUPS = 4
MESH = pl.DeviceIdType.MESH


rope_base = 10000.0
norm_eps = 1e-06


def shifted(block, axis, distance):
    devices = range(lax.axis_size(axis))
    route = [(i - distance, i) for i in devices if i - distance in devices]
    return lax.ppermute(block, axis, route)


def rotate(rows, positions, heads):
    half_dim = HDIM // 2
    values = rows.astype(jnp.float32).reshape(rows.shape[0], heads, HDIM)
    inverse = rope_base ** (-jnp.arange(half_dim, dtype=jnp.float32) / half_dim)
    angles = positions.astype(jnp.float32)[:, None] * inverse[None, :]
    cosines = jnp.cos(angles)[:, None, :]
    sines = jnp.sin(angles)[:, None, :]
    lower = values[..., :half_dim]
    upper = values[..., half_dim:]
    turned = jnp.concatenate(
        [lower * cosines - upper * sines, upper * cosines + lower * sines], axis=-1
    )
    return turned.reshape(rows.shape[0], heads * HDIM).astype(jnp.bfloat16)


ORDER = (0, 1, 2, 3)
LAST = 3
PIECES = 8
EARLY = 4
PARTS = 4


def layer_kernel(
    q_ref, k_ref, v_ref, inv_ref, sink_ref, w_ref, res_ref, gain_ref, routes_t_ref, rw_t_ref, gate_ref, up_ref,
    down_ref, out_ref,
    wbuf, abuf, acc, xs, rres, aps, rat, own_r, own_a, acc0, tok, gate_v, up_v, down_v, hid, y, yr, sum0, sum2, xrec, zsend, zrec,
    meta, meta_rx, pt_ref, stream_v, kv, rq, heads_v, cos_ref, sin_ref,
    lsem, wss, wrs, kss, krs, ass_, ars, mss, mrs, zss, zrs, oss, ors, dss, drs, rss, rrs,
):
    grp = lax.axis_index("grp")
    sp = lax.axis_index("sp")
    tp = lax.axis_index("tp")
    n_sp = GROUPS
    n_tp = 4
    rows = res_ref.shape[0]
    width = res_ref.shape[1]
    cap = xs.shape[1]
    epg = n_tp
    ff = gate_ref.shape[1]

    def sp_at(d):
        return lax.bitwise_xor(sp, d)

    near = tp + 1 - 2 * lax.rem(tp, 2)

    def tp_at(k):
        base = near if k % 2 else tp
        return lax.rem(base + 2, n_tp) if k >= 2 else base

    depth = w_ref.shape[0]

    def w_at(k):
        return wbuf.at[pl.ds(k * depth, depth)]

    local = [
        pltpu.make_async_copy(w_ref, w_at(0), lsem.at[0]),
        pltpu.make_async_copy(gate_ref, gate_v, lsem.at[1]),
        pltpu.make_async_copy(up_ref, up_v, lsem.at[2]),
        pltpu.make_async_copy(down_ref, down_v, lsem.at[3]),
    ]
    for c in local:
        c.start()

    barrier = pltpu.get_barrier_semaphore()
    for d in range(n_sp):
        for k in range(n_tp):
            if d or k:
                pl.semaphore_signal(
                    barrier, inc=1, device_id={"sp": sp_at(d), "tp": tp_at(k)},
                    device_id_type=MESH,
                )
    pl.semaphore_signal(
        barrier, inc=1, device_id={"grp": 1 - grp}, device_id_type=MESH
    )

    f32 = jnp.float32
    bf = jnp.bfloat16
    toks = q_ref.shape[0]
    half_dim = HDIM // 2
    lane_t = lax.broadcasted_iota(jnp.int32, (toks, 128), 1)
    lower = lax.rem(lane_t, HDIM) < half_dim

    def turn(x):
        other = jnp.where(
            lower, pltpu.roll(x, 128 - half_dim, 1), pltpu.roll(x, half_dim, 1)
        )
        return x * cos_ref[...] + other * sin_ref[...]

    pos = lax.broadcasted_iota(jnp.int32, (toks, 128), 0) + sp * toks
    angle = pos.astype(f32) * inv_ref[...]
    cos_ref[...] = jnp.cos(angle)
    sines = jnp.sin(angle)
    sin_ref[...] = jnp.where(lower, -sines, sines)
    both = jnp.concatenate([k_ref[...], v_ref[...]], axis=0).T
    turned = turn(both.astype(f32)).astype(bf)
    kv[WINDOW:, :] = jnp.where(lane_t < HDIM, turned, both)
    pl.semaphore_wait(barrier, n_sp * n_tp)

    sends = []

    def plan(src, dst, ssem, rsem, where):
        c = pltpu.make_async_remote_copy(
            src_ref=src, dst_ref=dst, send_sem=ssem, recv_sem=rsem,
            device_id=where, device_id_type=MESH,
        )
        sends.append(c)
        return c

    def post(src, dst, ssem, rsem, where):
        c = plan(src, dst, ssem, rsem, where)
        c.start()
        return c

    def send(src, dst, ssem, rsem, d, k):
        return post(src, dst, ssem, rsem, {"sp": sp_at(d), "tp": tp_at(k)})

    tail = post(
        kv.at[pl.ds(toks, WINDOW)], kv.at[pl.ds(0, WINDOW)], kss, krs,
        {"sp": lax.rem(sp + 1, n_sp)},
    )
    chunk = depth // (2 * PIECES)

    def w_rows(k, half, c):
        return pl.ds(pl.multiple_of(k * depth + half * (depth // 2) + c * chunk, chunk), chunk)

    w_far = []

    def w_open(c):
        w_far.append(
            send(
                wbuf.at[w_rows(0, grp, c)], wbuf.at[w_rows(2, grp, c)], wss.at[0, c], wrs.at[0, c], 0, 2
            )
        )

    w_side, w_last = [], []

    def w_cross(c):
        w_far[c].wait_recv()
        mine = wbuf.at[w_rows(2, grp, c)]
        w_side.append(post(mine, mine, wss.at[1, c], wrs.at[1, c], {"grp": 1 - grp}))
        w_last.append(send(mine, wbuf.at[w_rows(3, grp, c)], wss.at[2, c], wrs.at[2, c], 0, 1))

    def w_close(c):
        w_side[c].wait_recv()
        w_last.append(
            send(
                wbuf.at[w_rows(2, 1 - grp, c)], wbuf.at[w_rows(3, 1 - grp, c)], wss.at[3, c],
                wrs.at[3, c], 0, 1,
            )
        )

    local[0].wait()
    for c in range(EARLY):
        w_open(c)
    w_near = send(w_at(0), w_at(1), wss.at[4, 0], wrs.at[4, 0], 0, 1)

    ii = lax.broadcasted_iota(jnp.int32, (rows, rows), 0)
    jj = lax.broadcasted_iota(jnp.int32, (rows, rows), 1)
    low = jnp.where(jj < ii, 1.0, 0.0).astype(bf)
    upp = jnp.where(ii < jj, 1.0, 0.0).astype(bf)

    def relative(first):
        return lax.bitwise_xor(first, jnp.broadcast_to(sp * epg, first.shape))

    lane = lax.broadcasted_iota(jnp.int32, (rows, 128), 1)
    rel_r = relative(routes_t_ref[0:1, :])
    rel_r2 = relative(routes_t_ref[1:2, :])
    rel_c = jnp.sum(jnp.where(ii == jj, rel_r, 0), axis=1, keepdims=True)
    hot_c = jnp.where((rel_c >= lane * epg) & (rel_c < (lane + 1) * epg), 1.0, 0.0)
    rank_c = jnp.dot(low, hot_c.astype(bf), preferred_element_type=f32)
    lane_f = lane.astype(f32)
    slot_c = jnp.sum(hot_c * (lane_f * cap + rank_c), axis=1, keepdims=True)
    wide_c = jnp.sum(hot_c * (lane_f * 128 + rank_c), axis=1, keepdims=True)
    lane_s = lax.broadcasted_iota(jnp.int32, (rows, n_sp * cap), 1).astype(f32)
    pt_ref[...] = jnp.where(lane_s == slot_c, 1.0, 0.0).astype(bf)
    lane_w = lax.broadcasted_iota(jnp.int32, (rows, n_sp * 128), 1).astype(f32)
    pt_wide = jnp.where(lane_w == wide_c, 1.0, 0.0).astype(bf)

    sub = lax.broadcasted_iota(jnp.int32, (16, rows), 0)
    sub_f = sub.astype(f32)
    hot_r = jnp.where((rel_r >= sub * epg) & (rel_r < (sub + 1) * epg), 1.0, 0.0)
    rank_r = jnp.dot(hot_r.astype(bf), upp, preferred_element_type=f32)
    slot_r = jnp.sum(hot_r * (sub_f * cap + rank_r), axis=0, keepdims=True)
    group_r = jnp.sum(hot_r * sub_f, axis=0, keepdims=True)
    sub_s = lax.broadcasted_iota(jnp.int32, (cap, rows), 0).astype(f32)

    def chosen(d):
        return jnp.where(sub_s + float(d * cap) == slot_r, 1.0, 0.0).astype(bf)

    far = {}

    def send_rows(d):
        picked = jnp.dot(chosen(d), res_ref[...], preferred_element_type=f32).astype(bf)
        if d == 0:
            own_r[0] = picked
            return
        if d == LAST:
            rres[d] = picked
            return
        xs[d] = picked
        far[0, d] = send(xs.at[d], rres.at[d], zss.at[0, d], zrs.at[0, d], d, 0)

    own = {}

    def own_cast(kind, src, dst, via):
        buf = own_a if kind else own_r
        own[kind, dst] = send(
            buf.at[src], buf.at[dst], oss.at[kind, dst], ors.at[kind, dst], 0, via
        )

    send_rows(1)
    send_rows(2)
    send_rows(0)
    own_cast(0, 0, 1, 1)

    for j in range(q_ref.shape[1] // 128):
        cs = pl.ds(j * 128, 128)
        rq[:, cs] = turn(q_ref[:, cs].astype(f32)).astype(bf)

    first_r = rel_r.astype(f32) - epg * group_r
    second_r = rel_r2.astype(f32) - epg * group_r
    w_t = jnp.where(first_r == sub_f, rw_t_ref[0:1, :], 0.0) + jnp.where(
        second_r == sub_f, rw_t_ref[1:2, :], 0.0
    )
    hi = w_t.astype(bf)
    rest = w_t - hi.astype(f32)
    mid = rest.astype(bf)
    lo = (rest - mid.astype(f32)).astype(bf)
    placed = (
        jnp.dot(hi, pt_wide, preferred_element_type=f32)
        + jnp.dot(mid, pt_wide, preferred_element_type=f32)
        + jnp.dot(lo, pt_wide, preferred_element_type=f32)
    )
    for d in range(n_sp):
        meta[d] = placed[0:8, d * 128 : (d + 1) * 128]
    meta_rx[0, 0] = placed[0:8, 0:128]
    metas = {}
    for d in range(n_sp):
        for k in range(n_tp):
            if d or k:
                metas[d, k] = send(
                    meta.at[d], meta_rx.at[d, k], mss.at[d, k], mrs.at[d, k], d, k
                )

    n_heads = q_ref.shape[1] // HDIM
    tail.wait_recv()
    qi = lax.broadcasted_iota(jnp.int32, (WINDOW, 2 * WINDOW), 0)
    ki = lax.broadcasted_iota(jnp.int32, (WINDOW, 2 * WINDOW), 1)
    band = (ki > qi) & (ki <= qi + WINDOW)

    def attend(k):
        n = tp_at(k)
        start = pl.multiple_of(n * WINDOW, WINDOW)
        keys = kv[pl.ds(start, 2 * WINDOW), 0:HDIM]
        vals = kv[pl.ds(start, 2 * WINDOW), HDIM : 2 * HDIM]
        q = rq[pl.ds(start, WINDOW), :]
        first = jnp.where((sp == 0) & (n == 0), WINDOW, 0)
        seen = band & (ki >= first)
        outs = []
        for h in range(n_heads):
            sc = lax.dot_general(
                q[:, h * HDIM : (h + 1) * HDIM], keys, (((1,), (1,)), ((), ())),
                preferred_element_type=f32,
            ) * HDIM ** (-0.5)
            sc = jnp.where(seen, sc, -jnp.inf)
            sink = sink_ref[0:1, h : h + 1]
            top = jnp.maximum(jnp.max(sc, axis=1, keepdims=True), sink)
            e = jnp.exp(sc - top)
            den = jnp.sum(e, axis=1, keepdims=True) + jnp.exp(sink - top)
            pr = (e * (1.0 / den)).astype(bf)
            outs.append(jnp.dot(pr, vals, preferred_element_type=f32))
        heads_v[k] = jnp.concatenate(outs, axis=1).astype(bf)

    heads = {}

    def send_heads(k):
        heads[k] = send(heads_v.at[k], abuf.at[k], ass_.at[k], ars.at[k], 0, k)

    tile = width // 4

    def project(d):
        def step(i, _):
            cols = pl.ds(pl.multiple_of(i * tile, tile), tile)
            acc[:, cols] = jnp.dot(rat[d], wbuf[:, cols], preferred_element_type=f32)
            return 0

        lax.fori_loop(0, 4, step, 0)

    def pack_heads(k):
        block = abuf[k] if k else heads_v[0]
        cs = pl.ds(k * depth, depth)
        for d in ORDER:
            picked = jnp.dot(chosen(d), block, preferred_element_type=f32).astype(bf)
            if d == LAST:
                rat[d, :, cs] = picked
            elif d:
                aps[d, :, cs] = picked
            else:
                own_a[0, :, cs] = picked

    def send_heads_far(d):
        far[1, d] = send(aps.at[d], rat.at[d], zss.at[1, d], zrs.at[1, d], d, 0)

    attend(2)
    send_heads(2)
    w_cross(0)
    attend(3)
    send_heads(3)
    for c in range(EARLY, PIECES):
        w_open(c)
    own_cast(0, 0, 2, 2)
    w_cross(1)
    attend(1)
    send_heads(1)
    w_cross(2)
    w_close(0)
    attend(0)
    w_cross(3)
    w_close(1)
    pack_heads(0)
    heads[1].wait_recv()
    pack_heads(1)
    w_close(2)
    heads[2].wait_recv()
    pack_heads(2)
    heads[3].wait_recv()
    pack_heads(3)
    send_heads_far(1)
    send_heads_far(2)
    own_cast(1, 0, 1, 1)
    own_cast(1, 0, 2, 2)
    send_rows(LAST)
    w_near.wait_recv()
    w_cross(4)
    w_close(3)
    w_cross(5)
    w_cross(6)
    w_cross(7)
    w_close(4)
    w_close(5)
    w_close(6)
    w_close(7)
    for c in w_last:
        c.wait_recv()

    def shift(kind, _):
        own[kind, 2].wait_recv()
        own_cast(kind, 2, 3, 1)

    def gather(_, __):
        for kind in range(2):
            own[kind, 1].wait_recv()
            own[kind, 3].wait_recv()

        def step(t, _):
            cols = pl.ds(pl.multiple_of(t * tile, tile), tile)
            left = [
                jnp.concatenate(
                    [own_a[k, :, (i ^ k) * depth : ((i ^ k) + 1) * depth] for i in range(n_tp)], axis=1
                )
                for k in range(n_tp)
            ]
            acc0[:, cols] = jnp.dot(
                jnp.concatenate(left, axis=0), wbuf[:, cols], preferred_element_type=f32
            )
            return 0

        lax.fori_loop(0, 4, step, 0)
        for k in range(n_tp):
            settle(0, k, own_r[k], acc0[k * cap : (k + 1) * cap])

    def settle(d, k, rest, total):
        stream = (rest.astype(f32) + total).astype(bf)
        if k == 0:
            stream_v[d] = stream
        stream_f = stream.astype(f32)
        scale = lax.rsqrt(jnp.mean(stream_f * stream_f, axis=-1, keepdims=True) + norm_eps)
        normed = (stream_f * scale * gain_ref[...]).astype(bf)
        if d == LAST:
            xs[d] = normed
        else:
            tok[d, k] = normed

    ready = {}

    def norm_far(d, _):
        project(d)
        settle(d, 0, rres[d], acc[...])
        for h in range(PARTS):
            ready[h] = send(
                xs.at[d, :, part(h)], tok.at[d, 0, :, part(h)], dss.at[0, d, h], drs.at[0, d, h], d, 0
            )

    def pass_on(d, h):
        ready[h].wait_recv()
        cast(0, 2, d, h, 2)
        cast(0, 1, d, h, 1)

    half_w = width // PARTS

    def part(h):
        return pl.ds(h * half_w, half_w)

    plane = {}

    def cast(src, dst, d, h, via):
        plane[dst, d, h] = send(
            tok.at[d, src, :, part(h)], tok.at[d, dst, :, part(h)], dss.at[dst, d, h],
            drs.at[dst, d, h], 0, via,
        )

    def spread(d, _):
        far[0, d].wait_recv()
        far[1, d].wait_recv()
        project(d)
        settle(d, 0, rres[d], acc[...])
        for h in range(PARTS):
            cast(0, 2, d, h, 2)
            cast(0, 1, d, h, 1)

    def relay(d, h):
        plane[2, d, h].wait_recv()
        cast(2, 3, d, h, 1)

    eye = lax.broadcasted_iota(jnp.int32, (cap, 128), 0) == lax.broadcasted_iota(
        jnp.int32, (cap, 128), 1
    )
    f_tile = ff // 2
    back = {}

    def serve(d, _):
        cols = []
        if d:
            for h in range(PARTS):
                plane[1, d, h].wait_recv()
                plane[3, d, h].wait_recv()
        for k in range(n_tp):
            if d or k:
                metas[d, k].wait_recv()
            row = meta_rx[d, k, pl.ds(tp, 1), :]
            cols.append(jnp.sum(jnp.where(eye, row, 0.0), axis=1, keepdims=True))
        weight = jnp.concatenate(cols, axis=0)

        def inner(i, _):
            cs = pl.ds(pl.multiple_of(i * f_tile, f_tile), f_tile)
            x = tok[d].reshape(n_tp * cap, width)
            g = jnp.dot(x, gate_v[:, cs], preferred_element_type=f32)
            u = jnp.dot(x, up_v[:, cs], preferred_element_type=f32)
            hid[:, cs] = (g / (1.0 + jnp.exp(-g)) * u * weight).astype(bf)
            return 0

        lax.fori_loop(0, 2, inner, 0)
        def outer(i, _):
            cs = pl.ds(pl.multiple_of(i * tile, tile), tile)
            o = jnp.dot(hid[...], down_v[:, cs], preferred_element_type=f32).astype(bf)
            y[d, :, :, cs] = o.reshape(n_tp, cap, tile)
            return 0

        per = 4 // PARTS
        for h in range(PARTS):
            lax.fori_loop(h * per, (h + 1) * per, outer, 0)
            for k, slot in ((3, 1), (1, 0)):
                back[k, d, h] = send(
                    y.at[d, k, :, part(h)], yr.at[d, slot, :, part(h)], rss.at[slot, d, h],
                    rrs.at[slot, d, h], 0, 1,
                )

    def pair(d, h):
        cs = part(h)
        back[3, d, h].wait_recv()
        sum2[d, :, cs] = (y[d, 2, :, cs].astype(f32) + yr[d, 1, :, cs].astype(f32)).astype(bf)
        back[2, d, h] = send(
            sum2.at[d, :, cs], xrec.at[d, :, cs], rss.at[2, d, h], rrs.at[2, d, h], 0, 2
        )
        back[1, d, h].wait_recv()
        sum0[d, :, cs] = y[d, 0, :, cs].astype(f32) + yr[d, 0, :, cs].astype(f32)

    home = {}

    def finish(d, h):
        cs = part(h)
        back[2, d, h].wait_recv()
        total = sum0[d, :, cs] + xrec[d, :, cs].astype(f32)
        if d != LAST:
            total = total + stream_v[d, :, cs].astype(f32)
        total = total.astype(bf)
        if d:
            zsend[d, :, cs] = total
            home[d, h] = send(
                zsend.at[d, :, cs], zrec.at[d, :, cs], rss.at[3, d, h], rrs.at[3, d, h],
                d, 0,
            )
        else:
            zrec[0, :, cs] = total

    steps = (
        (spread, 2, 0),
        (norm_far, 3, 0),
        (spread, 1, 0),
        (shift, 0, 0),
        (shift, 1, 0),
        (gather, 0, 0),
        (relay, 2, 0),
        (relay, 2, 1),
        (relay, 2, 2),
        (relay, 2, 3),
        (serve, 2, 0),
        (pair, 2, 0),
        (pair, 2, 1),
        (pair, 2, 2),
        (pair, 2, 3),
        (relay, 1, 0),
        (relay, 1, 1),
        (relay, 1, 2),
        (relay, 1, 3),
        (pass_on, 3, 0),
        (pass_on, 3, 1),
        (pass_on, 3, 2),
        (pass_on, 3, 3),
        (serve, 1, 0),
        (pair, 1, 0),
        (pair, 1, 1),
        (pair, 1, 2),
        (pair, 1, 3),
        (finish, 2, 0),
        (finish, 2, 1),
        (serve, 0, 0),
        (finish, 2, 2),
        (finish, 2, 3),
        (relay, 3, 0),
        (relay, 3, 1),
        (relay, 3, 2),
        (relay, 3, 3),
        (serve, 3, 0),
        (pair, 3, 0),
        (finish, 1, 0),
        (pair, 3, 1),
        (finish, 1, 1),
        (pair, 3, 2),
        (finish, 1, 2),
        (pair, 3, 3),
        (finish, 1, 3),
        (pair, 0, 0),
        (finish, 3, 0),
        (pair, 0, 1),
        (finish, 3, 1),
        (pair, 0, 2),
        (finish, 3, 2),
        (pair, 0, 3),
        (finish, 3, 3),
        (finish, 0, 0),
        (finish, 0, 1),
        (finish, 0, 2),
        (finish, 0, 3),
    )
    for c in local[1:]:
        c.wait()
    for stage, d, h in steps:
        stage(d, h)
    def close(i, _):
        cs = pl.ds(pl.multiple_of(i * tile, tile), tile)
        last = (zrec[LAST, :, cs].astype(f32) + stream_v[LAST, :, cs].astype(f32)).astype(bf)
        rec = jnp.concatenate([zrec[d, :, cs] for d in range(LAST)] + [last], axis=0)
        got = jnp.dot(pt_ref[...], rec, preferred_element_type=f32)
        out_ref[:, cs] = got.astype(bf)
        return 0

    for h in range(PARTS):
        for d in ORDER[1:]:
            home[d, h].wait_recv()
        lax.fori_loop(h * 4 // PARTS, (h + 1) * 4 // PARTS, close, 0)
    for c in sends:
        c.wait_send()


def whole_layer(
    query_rows, key_rows, value_rows, sink_logits, residual, out_weight, norm_gain, gate_weight, up_weight, down_weight, routes,
    route_weight,
):
    n_tp = lax.axis_size("tp")
    n_sp = lax.axis_size("sp")
    rows, width = residual.shape
    ff = gate_weight.shape[2]
    depth = out_weight.shape[0]
    cap = 2 * rows // n_sp
    toks = query_rows.shape[0]
    half_dim = HDIM // 2
    inverse = rope_base ** (-np.arange(half_dim, dtype=np.float32) / np.float32(half_dim))
    table = np.tile(inverse.astype(np.float32), 4)[None, :]
    bf = jnp.bfloat16
    f32 = jnp.float32
    dma = pltpu.SemaphoreType.DMA
    vm = pl.BlockSpec(memory_space=pltpu.VMEM)
    hbm = pl.BlockSpec(memory_space=pl.ANY)
    return pl.pallas_call(
        layer_kernel,
        out_shape=jax.ShapeDtypeStruct((rows, width), bf),
        in_specs=[vm] * 5 + [hbm, vm, vm, vm, vm, hbm, hbm, hbm],
        out_specs=vm,
        scratch_shapes=[
            pltpu.VMEM((n_tp * depth, width), bf),
            pltpu.VMEM((n_tp, rows, depth), bf),
            pltpu.VMEM((cap, width), f32),
            pltpu.VMEM((n_sp, cap, width), bf),
            pltpu.VMEM((n_sp, cap, width), bf),
            pltpu.VMEM((n_sp, cap, n_tp * depth), bf),
            pltpu.VMEM((n_sp, cap, n_tp * depth), bf),
            pltpu.VMEM((n_tp, cap, width), bf),
            pltpu.VMEM((n_tp, cap, n_tp * depth), bf),
            pltpu.VMEM((n_tp * cap, width), f32),
            pltpu.VMEM((n_sp, n_tp, cap, width), bf),
            pltpu.VMEM((width, ff), bf),
            pltpu.VMEM((width, ff), bf),
            pltpu.VMEM((ff, width), bf),
            pltpu.VMEM((n_tp * cap, ff), bf),
            pltpu.VMEM((n_sp, n_tp, cap, width), bf),
            pltpu.VMEM((n_sp, 2, cap, width), bf),
            pltpu.VMEM((n_sp, cap, width), f32),
            pltpu.VMEM((n_sp, cap, width), bf),
            pltpu.VMEM((n_sp, cap, width), bf),
            pltpu.VMEM((n_sp, cap, width), bf),
            pltpu.VMEM((n_sp, cap, width), bf),
            pltpu.VMEM((n_sp, 8, 128), f32),
            pltpu.VMEM((n_sp, n_tp, 8, 128), f32),
            pltpu.VMEM((rows, n_sp * cap), bf),
            pltpu.VMEM((n_sp, cap, width), bf),
            pltpu.VMEM((toks + WINDOW, 2 * HDIM), bf),
            pltpu.VMEM((toks, depth), bf),
            pltpu.VMEM((n_tp, rows, depth), bf),
            pltpu.VMEM((toks, 128), f32),
            pltpu.VMEM((toks, 128), f32),
            dma((4,)), dma((5, PIECES)), dma((5, PIECES)), dma, dma, dma((4,)), dma((4,)),
            dma((n_sp, n_tp)), dma((n_sp, n_tp)), dma((2, n_sp)), dma((2, n_sp)),
            dma((2, n_tp)), dma((2, n_tp)),
            dma((4, n_sp, PARTS)), dma((4, n_sp, PARTS)), dma((4, n_sp, PARTS)),
            dma((4, n_sp, PARTS)),
        ],
        compiler_params=pltpu.CompilerParams(
            collective_id=0, has_side_effects=True, vmem_limit_bytes=60000 * 1024
        ),
        name="routed_layer",
    )(
        query_rows, key_rows.T, value_rows.T, jnp.asarray(table), sink_logits[None, :],
        out_weight,
        residual, norm_gain[None, :],
        routes.T, route_weight.T, gate_weight[0], up_weight[0], down_weight[0],
    )


def per_device(
    query_rows,
    key_rows,
    value_rows,
    sink_logits,
    residual,
    out_weight,
    norm_gain,
    gate_weight,
    up_weight,
    down_weight,
    routes,
    route_weight,
):
    tok_count = query_rows.shape[0]
    fits = (
        lax.axis_size("grp") == 2
        and lax.axis_size("sp") == GROUPS
        and lax.axis_size("tp") == 4
        and residual.shape[0] == WINDOW
        and key_rows.shape[1] == HDIM
        and query_rows.shape[1] % 128 == 0
    )
    if fits:
        return whole_layer(
            query_rows, key_rows, value_rows, sink_logits, residual, out_weight, norm_gain,
            gate_weight, up_weight, down_weight, routes, route_weight,
        )
    head_local = query_rows.shape[1] // HDIM
    group_local = key_rows.shape[1] // HDIM
    repeat = head_local // group_local
    first_pos = lax.axis_index("sp") * tok_count
    positions = first_pos + jnp.arange(tok_count, dtype=jnp.int32)
    rot_q = rotate(query_rows, positions, head_local)
    rot_k = rotate(key_rows, positions, group_local)
    tails = jnp.stack([rot_k[tok_count - WINDOW :], value_rows[tok_count - WINDOW :]])
    earlier = shifted(tails, "sp", 1)
    blocks = tok_count // WINDOW
    q_blocks = rot_q.reshape(blocks, WINDOW, group_local, repeat, HDIM)
    k_blocks = rot_k.reshape(blocks, WINDOW, group_local, HDIM)
    v_blocks = value_rows.reshape(blocks, WINDOW, group_local, HDIM)
    k_prev = jnp.concatenate(
        [earlier[0].reshape(1, WINDOW, group_local, HDIM), k_blocks[:-1]], axis=0
    )
    v_prev = jnp.concatenate(
        [earlier[1].reshape(1, WINDOW, group_local, HDIM), v_blocks[:-1]], axis=0
    )
    k_wide = jnp.concatenate([k_prev, k_blocks], axis=1)
    v_wide = jnp.concatenate([v_prev, v_blocks], axis=1)
    query_pos = jnp.arange(WINDOW) + WINDOW
    key_pos = jnp.arange(2 * WINDOW)
    distance = query_pos[:, None] - key_pos[None, :]
    in_band = (distance >= 0) & (distance < WINDOW)
    key_global = (
        first_pos + jnp.arange(blocks)[:, None, None] * WINDOW + key_pos[None, None, :] - WINDOW
    )
    allowed = in_band[None] & (key_global >= 0)
    scores = jnp.einsum(
        "nqgrd,nkgd->grnqk", q_blocks, k_wide, preferred_element_type=jnp.float32
    ) * HDIM ** (-0.5)
    scores = jnp.where(allowed[None, None], scores, -jnp.inf)
    sink_here = sink_logits.reshape(group_local, repeat)[:, :, None, None, None]
    largest = jnp.maximum(scores.max(axis=-1, keepdims=True), sink_here)
    exp_scores = jnp.exp(scores - largest)
    denominator = exp_scores.sum(axis=-1, keepdims=True) + jnp.exp(sink_here - largest)
    probs = (exp_scores / denominator).astype(jnp.bfloat16)
    attended = jnp.einsum("grnqk,nkgd->nqgrd", probs, v_wide, preferred_element_type=jnp.float32)
    attended = attended.astype(jnp.bfloat16).reshape(tok_count, head_local * HDIM)
    row_count = residual.shape[0]
    token_rows = lax.all_to_all(attended, "tp", split_axis=0, concat_axis=1, tiled=True)
    projected = jnp.dot(
        token_rows,
        lax.all_gather(out_weight, "tp", axis=0, tiled=True),
        preferred_element_type=jnp.float32,
    )
    stream_f = (residual.astype(jnp.float32) + projected).astype(jnp.bfloat16).astype(jnp.float32)
    normed = (
        stream_f
        * lax.rsqrt(jnp.mean(stream_f * stream_f, axis=-1, keepdims=True) + norm_eps)
        * norm_gain[None, :]
    ).astype(jnp.bfloat16)
    sp_count = lax.axis_size("sp")
    tp_count = lax.axis_size("tp")
    expert_count = sp_count * tp_count
    capacity = 4 * row_count // expert_count
    width = normed.shape[1]
    flat_expert = routes.reshape(-1)
    one_hot = (flat_expert[:, None] == jnp.arange(expert_count, dtype=jnp.int32)[None, :]).astype(
        jnp.int32
    )
    slot_rank = jnp.sum((jnp.cumsum(one_hot, axis=0) - one_hot) * one_hot, axis=1)
    slot_index = flat_expert * capacity + slot_rank
    token_of = jnp.arange(2 * row_count, dtype=jnp.int32) // 2
    outgoing = (
        jnp.zeros((expert_count * capacity, width), jnp.bfloat16)
        .at[slot_index]
        .set(normed[token_of])
    )
    outgoing = outgoing.reshape(expert_count, capacity, width)
    arrived = lax.all_to_all(outgoing, ("sp", "tp"), split_axis=0, concat_axis=0, tiled=True)
    flat_rows = arrived.reshape(-1, width)
    gate_out = jnp.dot(flat_rows, gate_weight[0], preferred_element_type=jnp.float32)
    up_out = jnp.dot(flat_rows, up_weight[0], preferred_element_type=jnp.float32)
    hidden = (jax.nn.silu(gate_out) * up_out).astype(jnp.bfloat16)
    produced = jnp.dot(hidden, down_weight[0], preferred_element_type=jnp.float32).astype(
        jnp.bfloat16
    )
    returned = lax.all_to_all(
        produced.reshape(arrived.shape), ("sp", "tp"), split_axis=0, concat_axis=0, tiled=True
    )
    gathered = returned.reshape(expert_count * capacity, width)[slot_index].astype(jnp.float32)
    weighted = gathered * route_weight.reshape(-1)[:, None]
    combined = weighted.reshape(row_count, 2, width).sum(axis=1)
    return (stream_f + combined).astype(jnp.bfloat16)


def solution(mesh):
    in_specs = (
        P(("grp", "sp"), "tp"),
        P(("grp", "sp"), "tp"),
        P(("grp", "sp"), "tp"),
        P("tp"),
        P(("grp", "sp", "tp"), None),
        P("tp", None),
        P(),
        P(("sp", "tp"), None, None),
        P(("sp", "tp"), None, None),
        P(("sp", "tp"), None, None),
        P(("grp", "sp", "tp"), None),
        P(("grp", "sp", "tp"), None),
    )
    out_specs = P(("grp", "sp", "tp"), None)
    return jax.shard_map(
        per_device, mesh=mesh, in_specs=in_specs, out_specs=out_specs, check_vma=False
    )
```

```python
import functools

import jax
import jax.numpy as jnp
import numpy as np
from jax import lax
from jax.experimental import pallas as pl
from jax.experimental.pallas import tpu as pltpu
from jax.sharding import PartitionSpec as P

HDIM = 64
WINDOW = 128
GROUPS = 4
MESH = pl.DeviceIdType.MESH


rope_base = 10000.0
norm_eps = 1e-06


def shifted(block, axis, distance):
    devices = range(lax.axis_size(axis))
    route = [(i - distance, i) for i in devices if i - distance in devices]
    return lax.ppermute(block, axis, route)


def rotate(rows, positions, heads):
    half_dim = HDIM // 2
    values = rows.astype(jnp.float32).reshape(rows.shape[0], heads, HDIM)
    inverse = rope_base ** (-jnp.arange(half_dim, dtype=jnp.float32) / half_dim)
    angles = positions.astype(jnp.float32)[:, None] * inverse[None, :]
    cosines = jnp.cos(angles)[:, None, :]
    sines = jnp.sin(angles)[:, None, :]
    lower = values[..., :half_dim]
    upper = values[..., half_dim:]
    turned = jnp.concatenate(
        [lower * cosines - upper * sines, upper * cosines + lower * sines], axis=-1
    )
    return turned.reshape(rows.shape[0], heads * HDIM).astype(jnp.bfloat16)


ORDER = (0, 1, 2, 3)
LAST = 3
PIECES = 8
EARLY = 4
PARTS = 4


def layer_kernel(
    q_ref, k_ref, v_ref, inv_ref, sink_ref, w_ref, res_ref, gain_ref, routes_t_ref, rw_t_ref, gate_ref, up_ref,
    down_ref, out_ref,
    wbuf, abuf, acc, xs, rres, aps, rat, own_r, own_a, acc0, tok, gate_v, up_v, down_v, hid, y, yr, sum0, sum2, xrec, zsend, zrec,
    meta, meta_rx, pt_ref, stream_v, kv, rq, heads_v, cos_ref, sin_ref,
    lsem, wss, wrs, kss, krs, ass_, ars, mss, mrs, zss, zrs, oss, ors, gss, drs, rrs,
):
    grp = lax.axis_index("grp")
    sp = lax.axis_index("sp")
    tp = lax.axis_index("tp")
    n_sp = GROUPS
    n_tp = 4
    rows = res_ref.shape[0]
    width = res_ref.shape[1]
    cap = xs.shape[1]
    epg = n_tp
    ff = gate_ref.shape[1]

    def sp_at(d):
        return lax.bitwise_xor(sp, d)

    near = tp + 1 - 2 * lax.rem(tp, 2)

    def tp_at(k):
        base = near if k % 2 else tp
        return lax.rem(base + 2, n_tp) if k >= 2 else base

    depth = w_ref.shape[0]

    def w_at(k):
        return wbuf.at[pl.ds(k * depth, depth)]

    local = [
        pltpu.make_async_copy(w_ref, w_at(0), lsem.at[0]),
        pltpu.make_async_copy(gate_ref, gate_v, lsem.at[1]),
        pltpu.make_async_copy(up_ref, up_v, lsem.at[2]),
        pltpu.make_async_copy(down_ref, down_v, lsem.at[3]),
    ]
    for c in local:
        c.start()

    barrier = pltpu.get_barrier_semaphore()
    for d in range(n_sp):
        for k in range(n_tp):
            if d or k:
                pl.semaphore_signal(
                    barrier, inc=1, device_id={"sp": sp_at(d), "tp": tp_at(k)},
                    device_id_type=MESH,
                )
    pl.semaphore_signal(
        barrier, inc=1, device_id={"grp": 1 - grp}, device_id_type=MESH
    )

    f32 = jnp.float32
    bf = jnp.bfloat16
    toks = q_ref.shape[0]
    half_dim = HDIM // 2
    lane_t = lax.broadcasted_iota(jnp.int32, (toks, 128), 1)
    lower = lax.rem(lane_t, HDIM) < half_dim

    def turn(x):
        other = jnp.where(
            lower, pltpu.roll(x, 128 - half_dim, 1), pltpu.roll(x, half_dim, 1)
        )
        return x * cos_ref[...] + other * sin_ref[...]

    pos = lax.broadcasted_iota(jnp.int32, (toks, 128), 0) + sp * toks
    angle = pos.astype(f32) * inv_ref[...]
    cos_ref[...] = jnp.cos(angle)
    sines = jnp.sin(angle)
    sin_ref[...] = jnp.where(lower, -sines, sines)
    both = jnp.concatenate([k_ref[...], v_ref[...]], axis=0).T
    turned = turn(both.astype(f32)).astype(bf)
    kv[WINDOW:, :] = jnp.where(lane_t < HDIM, turned, both)
    pl.semaphore_wait(barrier, n_sp * n_tp)

    sends = []

    def plan(src, dst, ssem, rsem, where):
        c = pltpu.make_async_remote_copy(
            src_ref=src, dst_ref=dst, send_sem=ssem, recv_sem=rsem,
            device_id=where, device_id_type=MESH,
        )
        sends.append(c)
        return c

    def post(src, dst, ssem, rsem, where):
        c = plan(src, dst, ssem, rsem, where)
        c.start()
        return c

    def pool(src, dst, group, rsem, d, k):
        c = pltpu.make_async_remote_copy(
            src_ref=src, dst_ref=dst, send_sem=gss.at[group], recv_sem=rsem,
            device_id={"sp": sp_at(d), "tp": tp_at(k)}, device_id_type=MESH,
        )
        c.start()
        return c

    def send(src, dst, ssem, rsem, d, k):
        return post(src, dst, ssem, rsem, {"sp": sp_at(d), "tp": tp_at(k)})

    tail = post(
        kv.at[pl.ds(toks, WINDOW)], kv.at[pl.ds(0, WINDOW)], kss, krs,
        {"sp": lax.rem(sp + 1, n_sp)},
    )
    chunk = depth // (2 * PIECES)

    def w_rows(k, half, c):
        return pl.ds(pl.multiple_of(k * depth + half * (depth // 2) + c * chunk, chunk), chunk)

    w_far = []

    def w_open(c):
        w_far.append(
            send(
                wbuf.at[w_rows(0, grp, c)], wbuf.at[w_rows(2, grp, c)], wss.at[0, c], wrs.at[0, c], 0, 2
            )
        )

    w_side, w_last = [], []

    def w_cross(c):
        w_far[c].wait_recv()
        mine = wbuf.at[w_rows(2, grp, c)]
        w_side.append(post(mine, mine, wss.at[1, c], wrs.at[1, c], {"grp": 1 - grp}))
        w_last.append(send(mine, wbuf.at[w_rows(3, grp, c)], wss.at[2, c], wrs.at[2, c], 0, 1))

    def w_close(c):
        w_side[c].wait_recv()
        w_last.append(
            send(
                wbuf.at[w_rows(2, 1 - grp, c)], wbuf.at[w_rows(3, 1 - grp, c)], wss.at[3, c],
                wrs.at[3, c], 0, 1,
            )
        )

    local[0].wait()
    for c in range(EARLY):
        w_open(c)
    w_near = send(w_at(0), w_at(1), wss.at[4, 0], wrs.at[4, 0], 0, 1)

    ii = lax.broadcasted_iota(jnp.int32, (rows, rows), 0)
    jj = lax.broadcasted_iota(jnp.int32, (rows, rows), 1)
    low = jnp.where(jj < ii, 1.0, 0.0).astype(bf)
    upp = jnp.where(ii < jj, 1.0, 0.0).astype(bf)

    def relative(first):
        return lax.bitwise_xor(first, jnp.broadcast_to(sp * epg, first.shape))

    lane = lax.broadcasted_iota(jnp.int32, (rows, 128), 1)
    rel_r = relative(routes_t_ref[0:1, :])
    rel_r2 = relative(routes_t_ref[1:2, :])
    rel_c = jnp.sum(jnp.where(ii == jj, rel_r, 0), axis=1, keepdims=True)
    hot_c = jnp.where((rel_c >= lane * epg) & (rel_c < (lane + 1) * epg), 1.0, 0.0)
    rank_c = jnp.dot(low, hot_c.astype(bf), preferred_element_type=f32)
    lane_f = lane.astype(f32)
    slot_c = jnp.sum(hot_c * (lane_f * cap + rank_c), axis=1, keepdims=True)
    wide_c = jnp.sum(hot_c * (lane_f * 128 + rank_c), axis=1, keepdims=True)
    lane_s = lax.broadcasted_iota(jnp.int32, (rows, n_sp * cap), 1).astype(f32)
    pt_ref[...] = jnp.where(lane_s == slot_c, 1.0, 0.0).astype(bf)
    lane_w = lax.broadcasted_iota(jnp.int32, (rows, n_sp * 128), 1).astype(f32)
    pt_wide = jnp.where(lane_w == wide_c, 1.0, 0.0).astype(bf)

    sub = lax.broadcasted_iota(jnp.int32, (16, rows), 0)
    sub_f = sub.astype(f32)
    hot_r = jnp.where((rel_r >= sub * epg) & (rel_r < (sub + 1) * epg), 1.0, 0.0)
    rank_r = jnp.dot(hot_r.astype(bf), upp, preferred_element_type=f32)
    slot_r = jnp.sum(hot_r * (sub_f * cap + rank_r), axis=0, keepdims=True)
    group_r = jnp.sum(hot_r * sub_f, axis=0, keepdims=True)
    sub_s = lax.broadcasted_iota(jnp.int32, (cap, rows), 0).astype(f32)

    def chosen(d):
        return jnp.where(sub_s + float(d * cap) == slot_r, 1.0, 0.0).astype(bf)

    far = {}

    def send_rows(d):
        picked = jnp.dot(chosen(d), res_ref[...], preferred_element_type=f32).astype(bf)
        if d == 0:
            own_r[0] = picked
            return
        if d == LAST:
            rres[d] = picked
            return
        xs[d] = picked
        far[0, d] = send(xs.at[d], rres.at[d], zss.at[0, d], zrs.at[0, d], d, 0)

    own = {}

    def own_cast(kind, src, dst, via):
        buf = own_a if kind else own_r
        own[kind, dst] = send(
            buf.at[src], buf.at[dst], oss.at[kind, dst], ors.at[kind, dst], 0, via
        )

    send_rows(1)
    send_rows(2)
    send_rows(0)
    own_cast(0, 0, 1, 1)

    for j in range(q_ref.shape[1] // 128):
        cs = pl.ds(j * 128, 128)
        rq[:, cs] = turn(q_ref[:, cs].astype(f32)).astype(bf)

    first_r = rel_r.astype(f32) - epg * group_r
    second_r = rel_r2.astype(f32) - epg * group_r
    w_t = jnp.where(first_r == sub_f, rw_t_ref[0:1, :], 0.0) + jnp.where(
        second_r == sub_f, rw_t_ref[1:2, :], 0.0
    )
    hi = w_t.astype(bf)
    rest = w_t - hi.astype(f32)
    mid = rest.astype(bf)
    lo = (rest - mid.astype(f32)).astype(bf)
    placed = (
        jnp.dot(hi, pt_wide, preferred_element_type=f32)
        + jnp.dot(mid, pt_wide, preferred_element_type=f32)
        + jnp.dot(lo, pt_wide, preferred_element_type=f32)
    )
    for d in range(n_sp):
        meta[d] = placed[0:8, d * 128 : (d + 1) * 128]
    meta_rx[0, 0] = placed[0:8, 0:128]
    metas = {}
    for d in range(n_sp):
        for k in range(n_tp):
            if d or k:
                metas[d, k] = send(
                    meta.at[d], meta_rx.at[d, k], mss.at[d, k], mrs.at[d, k], d, k
                )

    n_heads = q_ref.shape[1] // HDIM
    tail.wait_recv()
    qi = lax.broadcasted_iota(jnp.int32, (WINDOW, 2 * WINDOW), 0)
    ki = lax.broadcasted_iota(jnp.int32, (WINDOW, 2 * WINDOW), 1)
    band = (ki > qi) & (ki <= qi + WINDOW)

    def attend(k):
        n = tp_at(k)
        start = pl.multiple_of(n * WINDOW, WINDOW)
        keys = kv[pl.ds(start, 2 * WINDOW), 0:HDIM]
        vals = kv[pl.ds(start, 2 * WINDOW), HDIM : 2 * HDIM]
        q = rq[pl.ds(start, WINDOW), :]
        first = jnp.where((sp == 0) & (n == 0), WINDOW, 0)
        seen = band & (ki >= first)
        outs = []
        for h in range(n_heads):
            sc = lax.dot_general(
                q[:, h * HDIM : (h + 1) * HDIM], keys, (((1,), (1,)), ((), ())),
                preferred_element_type=f32,
            ) * HDIM ** (-0.5)
            sc = jnp.where(seen, sc, -jnp.inf)
            sink = sink_ref[0:1, h : h + 1]
            top = jnp.maximum(jnp.max(sc, axis=1, keepdims=True), sink)
            e = jnp.exp(sc - top)
            den = jnp.sum(e, axis=1, keepdims=True) + jnp.exp(sink - top)
            pr = (e * (1.0 / den)).astype(bf)
            outs.append(jnp.dot(pr, vals, preferred_element_type=f32))
        heads_v[k] = jnp.concatenate(outs, axis=1).astype(bf)

    heads = {}

    def send_heads(k):
        heads[k] = send(heads_v.at[k], abuf.at[k], ass_.at[k], ars.at[k], 0, k)

    tile = width // 4

    def project(d):
        def step(i, _):
            cols = pl.ds(pl.multiple_of(i * tile, tile), tile)
            acc[:, cols] = jnp.dot(rat[d], wbuf[:, cols], preferred_element_type=f32)
            return 0

        lax.fori_loop(0, 4, step, 0)

    def pack_heads(k):
        block = abuf[k] if k else heads_v[0]
        cs = pl.ds(k * depth, depth)
        for d in ORDER:
            picked = jnp.dot(chosen(d), block, preferred_element_type=f32).astype(bf)
            if d == LAST:
                rat[d, :, cs] = picked
            elif d:
                aps[d, :, cs] = picked
            else:
                own_a[0, :, cs] = picked

    def send_heads_far(d):
        far[1, d] = send(aps.at[d], rat.at[d], zss.at[1, d], zrs.at[1, d], d, 0)

    attend(2)
    send_heads(2)
    w_cross(0)
    attend(3)
    send_heads(3)
    for c in range(EARLY, PIECES):
        w_open(c)
    own_cast(0, 0, 2, 2)
    w_cross(1)
    attend(1)
    send_heads(1)
    w_cross(2)
    w_close(0)
    attend(0)
    w_cross(3)
    w_close(1)
    pack_heads(0)
    heads[1].wait_recv()
    pack_heads(1)
    w_close(2)
    heads[2].wait_recv()
    pack_heads(2)
    heads[3].wait_recv()
    pack_heads(3)
    send_heads_far(1)
    send_heads_far(2)
    own_cast(1, 0, 1, 1)
    own_cast(1, 0, 2, 2)
    send_rows(LAST)
    w_near.wait_recv()
    w_cross(4)
    w_close(3)
    w_cross(5)
    w_cross(6)
    w_cross(7)
    w_close(4)
    w_close(5)
    w_close(6)
    w_close(7)
    for c in w_last:
        c.wait_recv()

    def shift(kind, _):
        own[kind, 2].wait_recv()
        own_cast(kind, 2, 3, 1)

    def gather(_, __):
        for kind in range(2):
            own[kind, 1].wait_recv()
            own[kind, 3].wait_recv()

        def step(t, _):
            cols = pl.ds(pl.multiple_of(t * tile, tile), tile)
            left = [
                jnp.concatenate(
                    [own_a[k, :, (i ^ k) * depth : ((i ^ k) + 1) * depth] for i in range(n_tp)], axis=1
                )
                for k in range(n_tp)
            ]
            acc0[:, cols] = jnp.dot(
                jnp.concatenate(left, axis=0), wbuf[:, cols], preferred_element_type=f32
            )
            return 0

        lax.fori_loop(0, 4, step, 0)
        for k in range(n_tp):
            settle(0, k, own_r[k], acc0[k * cap : (k + 1) * cap])

    def settle(d, k, rest, total):
        stream = (rest.astype(f32) + total).astype(bf)
        if k == 0:
            stream_v[d] = stream
        stream_f = stream.astype(f32)
        scale = lax.rsqrt(jnp.mean(stream_f * stream_f, axis=-1, keepdims=True) + norm_eps)
        normed = (stream_f * scale * gain_ref[...]).astype(bf)
        if d == LAST:
            xs[d] = normed
        else:
            tok[d, k] = normed

    ready = {}

    def norm_far(d, _):
        project(d)
        settle(d, 0, rres[d], acc[...])
        for h in range(PARTS):
            ready[h] = pool(xs.at[d, :, part(h)], tok.at[d, 0, :, part(h)], 0, drs.at[0, d, h], d, 0)

    def pass_on(d, h):
        ready[h].wait_recv()
        cast(0, 2, d, h, 2)
        cast(0, 1, d, h, 1)

    half_w = width // PARTS

    def part(h):
        return pl.ds(h * half_w, half_w)

    plane = {}

    def cast(src, dst, d, h, via):
        plane[dst, d, h] = pool(
            tok.at[d, src, :, part(h)], tok.at[d, dst, :, part(h)], 1, drs.at[dst, d, h], 0, via
        )

    def spread(d, _):
        far[0, d].wait_recv()
        far[1, d].wait_recv()
        project(d)
        settle(d, 0, rres[d], acc[...])
        for h in range(PARTS):
            cast(0, 2, d, h, 2)
            cast(0, 1, d, h, 1)

    def relay(d, h):
        plane[2, d, h].wait_recv()
        cast(2, 3, d, h, 1)

    eye = lax.broadcasted_iota(jnp.int32, (cap, 128), 0) == lax.broadcasted_iota(
        jnp.int32, (cap, 128), 1
    )
    f_tile = ff // 2
    back = {}

    def serve(d, _):
        cols = []
        if d:
            for h in range(PARTS):
                plane[1, d, h].wait_recv()
                plane[3, d, h].wait_recv()
        for k in range(n_tp):
            if d or k:
                metas[d, k].wait_recv()
            row = meta_rx[d, k, pl.ds(tp, 1), :]
            cols.append(jnp.sum(jnp.where(eye, row, 0.0), axis=1, keepdims=True))
        weight = jnp.concatenate(cols, axis=0)

        def inner(i, _):
            cs = pl.ds(pl.multiple_of(i * f_tile, f_tile), f_tile)
            x = tok[d].reshape(n_tp * cap, width)
            g = jnp.dot(x, gate_v[:, cs], preferred_element_type=f32)
            u = jnp.dot(x, up_v[:, cs], preferred_element_type=f32)
            hid[:, cs] = (g / (1.0 + jnp.exp(-g)) * u * weight).astype(bf)
            return 0

        lax.fori_loop(0, 2, inner, 0)
        def outer(i, _):
            cs = pl.ds(pl.multiple_of(i * tile, tile), tile)
            o = jnp.dot(hid[...], down_v[:, cs], preferred_element_type=f32).astype(bf)
            y[d, :, :, cs] = o.reshape(n_tp, cap, tile)
            return 0

        per = 4 // PARTS
        for h in range(PARTS):
            lax.fori_loop(h * per, (h + 1) * per, outer, 0)
            for k, slot in ((3, 1), (1, 0)):
                back[k, d, h] = pool(
                    y.at[d, k, :, part(h)], yr.at[d, slot, :, part(h)], 0, rrs.at[slot, d, h], 0, 1
                )

    def pair(d, h):
        cs = part(h)
        back[3, d, h].wait_recv()
        sum2[d, :, cs] = (y[d, 2, :, cs].astype(f32) + yr[d, 1, :, cs].astype(f32)).astype(bf)
        back[2, d, h] = pool(sum2.at[d, :, cs], xrec.at[d, :, cs], 0, rrs.at[2, d, h], 0, 2)
        back[1, d, h].wait_recv()
        sum0[d, :, cs] = y[d, 0, :, cs].astype(f32) + yr[d, 0, :, cs].astype(f32)

    home = {}

    def finish(d, h):
        cs = part(h)
        back[2, d, h].wait_recv()
        total = sum0[d, :, cs] + xrec[d, :, cs].astype(f32)
        if d != LAST:
            total = total + stream_v[d, :, cs].astype(f32)
        total = total.astype(bf)
        if d:
            zsend[d, :, cs] = total
            home[d, h] = pool(zsend.at[d, :, cs], zrec.at[d, :, cs], 0, rrs.at[3, d, h], d, 0)
        else:
            zrec[0, :, cs] = total

    inner_steps = (
        (spread, 2, 0),
        (norm_far, 3, 0),
        (spread, 1, 0),
        (shift, 0, 0),
        (shift, 1, 0),
        (gather, 0, 0),
        (relay, 2, 0),
        (relay, 2, 1),
        (relay, 2, 2),
        (relay, 2, 3),
        (serve, 2, 0),
        (pair, 2, 0),
        (pair, 2, 1),
        (pair, 2, 2),
        (pair, 2, 3),
        (relay, 1, 0),
        (relay, 1, 1),
        (relay, 1, 2),
        (relay, 1, 3),
        (pass_on, 3, 0),
        (pass_on, 3, 1),
        (pass_on, 3, 2),
        (pass_on, 3, 3),
        (serve, 1, 0),
        (pair, 1, 0),
        (pair, 1, 1),
        (pair, 1, 2),
        (pair, 1, 3),
        (finish, 2, 0),
        (finish, 2, 1),
        (serve, 0, 0),
        (finish, 2, 2),
        (finish, 2, 3),
        (relay, 3, 0),
        (relay, 3, 1),
        (relay, 3, 2),
        (relay, 3, 3),
        (serve, 3, 0),
        (pair, 3, 0),
        (finish, 1, 0),
        (pair, 3, 1),
        (finish, 1, 1),
        (pair, 3, 2),
        (finish, 1, 2),
        (pair, 3, 3),
        (finish, 1, 3),
        (pair, 0, 0),
        (finish, 3, 0),
        (pair, 0, 1),
        (finish, 3, 1),
        (pair, 0, 2),
        (finish, 3, 2),
        (pair, 0, 3),
        (finish, 3, 3),
        (finish, 0, 0),
        (finish, 0, 1),
        (finish, 0, 2),
        (finish, 0, 3),
    )
    outer_steps = (
        (spread, 2, 0),
        (norm_far, 3, 0),
        (spread, 1, 0),
        (shift, 0, 0),
        (shift, 1, 0),
        (gather, 0, 0),
        (relay, 2, 0),
        (relay, 2, 1),
        (relay, 2, 2),
        (relay, 2, 3),
        (serve, 2, 0),
        (pass_on, 3, 0),
        (pass_on, 3, 1),
        (pass_on, 3, 2),
        (pass_on, 3, 3),
        (pair, 2, 0),
        (pair, 2, 1),
        (pair, 2, 2),
        (pair, 2, 3),
        (relay, 1, 0),
        (relay, 1, 1),
        (relay, 1, 2),
        (relay, 1, 3),
        (serve, 1, 0),
        (relay, 3, 0),
        (relay, 3, 1),
        (relay, 3, 2),
        (relay, 3, 3),
        (serve, 3, 0),
        (finish, 2, 0),
        (finish, 2, 1),
        (pair, 3, 0),
        (pair, 3, 1),
        (pair, 3, 2),
        (pair, 3, 3),
        (finish, 2, 2),
        (finish, 2, 3),
        (pair, 1, 0),
        (pair, 1, 1),
        (pair, 1, 2),
        (pair, 1, 3),
        (finish, 3, 0),
        (serve, 0, 0),
        (finish, 3, 1),
        (finish, 3, 2),
        (finish, 3, 3),
        (pair, 0, 0),
        (pair, 0, 1),
        (pair, 0, 2),
        (pair, 0, 3),
        (finish, 1, 0),
        (finish, 1, 1),
        (finish, 1, 2),
        (finish, 1, 3),
        (finish, 0, 0),
        (finish, 0, 1),
        (finish, 0, 2),
        (finish, 0, 3),
    )
    for c in local[1:]:
        c.wait()

    def close(i, _):
        cs = pl.ds(pl.multiple_of(i * tile, tile), tile)
        last = (zrec[LAST, :, cs].astype(f32) + stream_v[LAST, :, cs].astype(f32)).astype(bf)
        rec = jnp.concatenate([zrec[d, :, cs] for d in range(LAST)] + [last], axis=0)
        got = jnp.dot(pt_ref[...], rec, preferred_element_type=f32)
        out_ref[:, cs] = got.astype(bf)
        return 0

    def rest(steps):
        before = list(sends)
        for stage, d, h in steps:
            stage(d, h)
        for h in range(PARTS):
            for d in ORDER[1:]:
                home[d, h].wait_recv()
            lax.fori_loop(h * 4 // PARTS, (h + 1) * 4 // PARTS, close, 0)
        for c in sends:
            c.wait_send()
        for group, span in enumerate((tok, tok.at[pl.ds(0, n_sp - 1), pl.ds(0, n_tp - 1)])):
            pltpu.make_async_remote_copy(
                src_ref=span, dst_ref=span, send_sem=gss.at[group], recv_sem=krs,
                device_id={"sp": sp_at(1), "tp": tp_at(0)}, device_id_type=MESH,
            ).wait_send()
        sends[:] = before

    inner = (sp == 1) | (sp == n_sp - 2)
    pl.when(inner)(functools.partial(rest, inner_steps))
    pl.when(jnp.logical_not(inner))(functools.partial(rest, outer_steps))


def whole_layer(
    query_rows, key_rows, value_rows, sink_logits, residual, out_weight, norm_gain, gate_weight, up_weight, down_weight, routes,
    route_weight,
):
    n_tp = lax.axis_size("tp")
    n_sp = lax.axis_size("sp")
    rows, width = residual.shape
    ff = gate_weight.shape[2]
    depth = out_weight.shape[0]
    cap = 2 * rows // n_sp
    toks = query_rows.shape[0]
    half_dim = HDIM // 2
    inverse = rope_base ** (-np.arange(half_dim, dtype=np.float32) / np.float32(half_dim))
    table = np.tile(inverse.astype(np.float32), 4)[None, :]
    bf = jnp.bfloat16
    f32 = jnp.float32
    dma = pltpu.SemaphoreType.DMA
    vm = pl.BlockSpec(memory_space=pltpu.VMEM)
    hbm = pl.BlockSpec(memory_space=pl.ANY)
    return pl.pallas_call(
        layer_kernel,
        out_shape=jax.ShapeDtypeStruct((rows, width), bf),
        in_specs=[vm] * 5 + [hbm, vm, vm, vm, vm, hbm, hbm, hbm],
        out_specs=vm,
        scratch_shapes=[
            pltpu.VMEM((n_tp * depth, width), bf),
            pltpu.VMEM((n_tp, rows, depth), bf),
            pltpu.VMEM((cap, width), f32),
            pltpu.VMEM((n_sp, cap, width), bf),
            pltpu.VMEM((n_sp, cap, width), bf),
            pltpu.VMEM((n_sp, cap, n_tp * depth), bf),
            pltpu.VMEM((n_sp, cap, n_tp * depth), bf),
            pltpu.VMEM((n_tp, cap, width), bf),
            pltpu.VMEM((n_tp, cap, n_tp * depth), bf),
            pltpu.VMEM((n_tp * cap, width), f32),
            pltpu.VMEM((n_sp, n_tp, cap, width), bf),
            pltpu.VMEM((width, ff), bf),
            pltpu.VMEM((width, ff), bf),
            pltpu.VMEM((ff, width), bf),
            pltpu.VMEM((n_tp * cap, ff), bf),
            pltpu.VMEM((n_sp, n_tp, cap, width), bf),
            pltpu.VMEM((n_sp, 2, cap, width), bf),
            pltpu.VMEM((n_sp, cap, width), f32),
            pltpu.VMEM((n_sp, cap, width), bf),
            pltpu.VMEM((n_sp, cap, width), bf),
            pltpu.VMEM((n_sp, cap, width), bf),
            pltpu.VMEM((n_sp, cap, width), bf),
            pltpu.VMEM((n_sp, 8, 128), f32),
            pltpu.VMEM((n_sp, n_tp, 8, 128), f32),
            pltpu.VMEM((rows, n_sp * cap), bf),
            pltpu.VMEM((n_sp, cap, width), bf),
            pltpu.VMEM((toks + WINDOW, 2 * HDIM), bf),
            pltpu.VMEM((toks, depth), bf),
            pltpu.VMEM((n_tp, rows, depth), bf),
            pltpu.VMEM((toks, 128), f32),
            pltpu.VMEM((toks, 128), f32),
            dma((4,)), dma((5, PIECES)), dma((5, PIECES)), dma, dma, dma((4,)), dma((4,)),
            dma((n_sp, n_tp)), dma((n_sp, n_tp)), dma((2, n_sp)), dma((2, n_sp)),
            dma((2, n_tp)), dma((2, n_tp)),
            dma((2,)), dma((4, n_sp, PARTS)), dma((4, n_sp, PARTS)),
        ],
        compiler_params=pltpu.CompilerParams(
            collective_id=0, has_side_effects=True, vmem_limit_bytes=60000 * 1024
        ),
        name="routed_layer",
    )(
        query_rows, key_rows.T, value_rows.T, jnp.asarray(table), sink_logits[None, :],
        out_weight,
        residual, norm_gain[None, :],
        routes.T, route_weight.T, gate_weight[0], up_weight[0], down_weight[0],
    )


def per_device(
    query_rows,
    key_rows,
    value_rows,
    sink_logits,
    residual,
    out_weight,
    norm_gain,
    gate_weight,
    up_weight,
    down_weight,
    routes,
    route_weight,
):
    tok_count = query_rows.shape[0]
    fits = (
        lax.axis_size("grp") == 2
        and lax.axis_size("sp") == GROUPS
        and lax.axis_size("tp") == 4
        and residual.shape[0] == WINDOW
        and key_rows.shape[1] == HDIM
        and query_rows.shape[1] % 128 == 0
    )
    if fits:
        return whole_layer(
            query_rows, key_rows, value_rows, sink_logits, residual, out_weight, norm_gain,
            gate_weight, up_weight, down_weight, routes, route_weight,
        )
    head_local = query_rows.shape[1] // HDIM
    group_local = key_rows.shape[1] // HDIM
    repeat = head_local // group_local
    first_pos = lax.axis_index("sp") * tok_count
    positions = first_pos + jnp.arange(tok_count, dtype=jnp.int32)
    rot_q = rotate(query_rows, positions, head_local)
    rot_k = rotate(key_rows, positions, group_local)
    tails = jnp.stack([rot_k[tok_count - WINDOW :], value_rows[tok_count - WINDOW :]])
    earlier = shifted(tails, "sp", 1)
    blocks = tok_count // WINDOW
    q_blocks = rot_q.reshape(blocks, WINDOW, group_local, repeat, HDIM)
    k_blocks = rot_k.reshape(blocks, WINDOW, group_local, HDIM)
    v_blocks = value_rows.reshape(blocks, WINDOW, group_local, HDIM)
    k_prev = jnp.concatenate(
        [earlier[0].reshape(1, WINDOW, group_local, HDIM), k_blocks[:-1]], axis=0
    )
    v_prev = jnp.concatenate(
        [earlier[1].reshape(1, WINDOW, group_local, HDIM), v_blocks[:-1]], axis=0
    )
    k_wide = jnp.concatenate([k_prev, k_blocks], axis=1)
    v_wide = jnp.concatenate([v_prev, v_blocks], axis=1)
    query_pos = jnp.arange(WINDOW) + WINDOW
    key_pos = jnp.arange(2 * WINDOW)
    distance = query_pos[:, None] - key_pos[None, :]
    in_band = (distance >= 0) & (distance < WINDOW)
    key_global = (
        first_pos + jnp.arange(blocks)[:, None, None] * WINDOW + key_pos[None, None, :] - WINDOW
    )
    allowed = in_band[None] & (key_global >= 0)
    scores = jnp.einsum(
        "nqgrd,nkgd->grnqk", q_blocks, k_wide, preferred_element_type=jnp.float32
    ) * HDIM ** (-0.5)
    scores = jnp.where(allowed[None, None], scores, -jnp.inf)
    sink_here = sink_logits.reshape(group_local, repeat)[:, :, None, None, None]
    largest = jnp.maximum(scores.max(axis=-1, keepdims=True), sink_here)
    exp_scores = jnp.exp(scores - largest)
    denominator = exp_scores.sum(axis=-1, keepdims=True) + jnp.exp(sink_here - largest)
    probs = (exp_scores / denominator).astype(jnp.bfloat16)
    attended = jnp.einsum("grnqk,nkgd->nqgrd", probs, v_wide, preferred_element_type=jnp.float32)
    attended = attended.astype(jnp.bfloat16).reshape(tok_count, head_local * HDIM)
    row_count = residual.shape[0]
    token_rows = lax.all_to_all(attended, "tp", split_axis=0, concat_axis=1, tiled=True)
    projected = jnp.dot(
        token_rows,
        lax.all_gather(out_weight, "tp", axis=0, tiled=True),
        preferred_element_type=jnp.float32,
    )
    stream_f = (residual.astype(jnp.float32) + projected).astype(jnp.bfloat16).astype(jnp.float32)
    normed = (
        stream_f
        * lax.rsqrt(jnp.mean(stream_f * stream_f, axis=-1, keepdims=True) + norm_eps)
        * norm_gain[None, :]
    ).astype(jnp.bfloat16)
    sp_count = lax.axis_size("sp")
    tp_count = lax.axis_size("tp")
    expert_count = sp_count * tp_count
    capacity = 4 * row_count // expert_count
    width = normed.shape[1]
    flat_expert = routes.reshape(-1)
    one_hot = (flat_expert[:, None] == jnp.arange(expert_count, dtype=jnp.int32)[None, :]).astype(
        jnp.int32
    )
    slot_rank = jnp.sum((jnp.cumsum(one_hot, axis=0) - one_hot) * one_hot, axis=1)
    slot_index = flat_expert * capacity + slot_rank
    token_of = jnp.arange(2 * row_count, dtype=jnp.int32) // 2
    outgoing = (
        jnp.zeros((expert_count * capacity, width), jnp.bfloat16)
        .at[slot_index]
        .set(normed[token_of])
    )
    outgoing = outgoing.reshape(expert_count, capacity, width)
    arrived = lax.all_to_all(outgoing, ("sp", "tp"), split_axis=0, concat_axis=0, tiled=True)
    flat_rows = arrived.reshape(-1, width)
    gate_out = jnp.dot(flat_rows, gate_weight[0], preferred_element_type=jnp.float32)
    up_out = jnp.dot(flat_rows, up_weight[0], preferred_element_type=jnp.float32)
    hidden = (jax.nn.silu(gate_out) * up_out).astype(jnp.bfloat16)
    produced = jnp.dot(hidden, down_weight[0], preferred_element_type=jnp.float32).astype(
        jnp.bfloat16
    )
    returned = lax.all_to_all(
        produced.reshape(arrived.shape), ("sp", "tp"), split_axis=0, concat_axis=0, tiled=True
    )
    gathered = returned.reshape(expert_count * capacity, width)[slot_index].astype(jnp.float32)
    weighted = gathered * route_weight.reshape(-1)[:, None]
    combined = weighted.reshape(row_count, 2, width).sum(axis=1)
    return (stream_f + combined).astype(jnp.bfloat16)


def solution(mesh):
    in_specs = (
        P(("grp", "sp"), "tp"),
        P(("grp", "sp"), "tp"),
        P(("grp", "sp"), "tp"),
        P("tp"),
        P(("grp", "sp", "tp"), None),
        P("tp", None),
        P(),
        P(("sp", "tp"), None, None),
        P(("sp", "tp"), None, None),
        P(("sp", "tp"), None, None),
        P(("grp", "sp", "tp"), None),
        P(("grp", "sp", "tp"), None),
    )
    out_specs = P(("grp", "sp", "tp"), None)
    return jax.shard_map(
        per_device, mesh=mesh, in_specs=in_specs, out_specs=out_specs, check_vma=False
    )
```

```python
import functools

import jax
import jax.numpy as jnp
import numpy as np
from jax import lax
from jax.experimental import pallas as pl
from jax.experimental.pallas import tpu as pltpu
from jax.sharding import PartitionSpec as P

HDIM = 64
WINDOW = 128
GROUPS = 4
MESH = pl.DeviceIdType.MESH


rope_base = 10000.0
norm_eps = 1e-06


def shifted(block, axis, distance):
    devices = range(lax.axis_size(axis))
    route = [(i - distance, i) for i in devices if i - distance in devices]
    return lax.ppermute(block, axis, route)


def rotate(rows, positions, heads):
    half_dim = HDIM // 2
    values = rows.astype(jnp.float32).reshape(rows.shape[0], heads, HDIM)
    inverse = rope_base ** (-jnp.arange(half_dim, dtype=jnp.float32) / half_dim)
    angles = positions.astype(jnp.float32)[:, None] * inverse[None, :]
    cosines = jnp.cos(angles)[:, None, :]
    sines = jnp.sin(angles)[:, None, :]
    lower = values[..., :half_dim]
    upper = values[..., half_dim:]
    turned = jnp.concatenate(
        [lower * cosines - upper * sines, upper * cosines + lower * sines], axis=-1
    )
    return turned.reshape(rows.shape[0], heads * HDIM).astype(jnp.bfloat16)


ORDER = (0, 1, 2, 3)
LAST = 3
PIECES = 8
EARLY = 4
PARTS = 4


def layer_kernel(
    q_ref, k_ref, v_ref, inv_ref, sink_ref, w_ref, res_ref, gain_ref, routes_t_ref, rw_t_ref, gate_ref, up_ref,
    down_ref, out_ref,
    wbuf, abuf, acc, xs, rres, aps, rat, own_r, own_a, acc0, tok, gate_v, up_v, down_v, hid, y, yr, sum0, sum2, xrec, zsend, zrec,
    meta, meta_rx, pt_ref, stream_v, kv, rq, heads_v, cos_ref, sin_ref,
    lsem, wss, wnr, wrs, kss, krs, ass_, ars, mss, mrs, zss, zrs, oss, ors, gss, drs, rrs,
):
    grp = lax.axis_index("grp")
    sp = lax.axis_index("sp")
    tp = lax.axis_index("tp")
    n_sp = GROUPS
    n_tp = 4
    rows = res_ref.shape[0]
    width = res_ref.shape[1]
    cap = xs.shape[1]
    epg = n_tp
    ff = gate_ref.shape[1]

    def sp_at(d):
        return lax.bitwise_xor(sp, d)

    near = tp + 1 - 2 * lax.rem(tp, 2)

    def tp_at(k):
        base = near if k % 2 else tp
        return lax.rem(base + 2, n_tp) if k >= 2 else base

    depth = w_ref.shape[0]

    def w_at(k):
        return wbuf.at[pl.ds(k * depth, depth)]

    local = [
        pltpu.make_async_copy(w_ref, w_at(0), lsem.at[0]),
        pltpu.make_async_copy(gate_ref, gate_v, lsem.at[1]),
        pltpu.make_async_copy(up_ref, up_v, lsem.at[2]),
        pltpu.make_async_copy(down_ref, down_v, lsem.at[3]),
    ]
    for c in local:
        c.start()

    barrier = pltpu.get_barrier_semaphore()
    for d in range(n_sp):
        for k in range(n_tp):
            if d or k:
                pl.semaphore_signal(
                    barrier, inc=1, device_id={"sp": sp_at(d), "tp": tp_at(k)},
                    device_id_type=MESH,
                )
    pl.semaphore_signal(
        barrier, inc=1, device_id={"grp": 1 - grp}, device_id_type=MESH
    )

    f32 = jnp.float32
    bf = jnp.bfloat16
    toks = q_ref.shape[0]
    half_dim = HDIM // 2
    lane_t = lax.broadcasted_iota(jnp.int32, (toks, 128), 1)
    lower = lax.rem(lane_t, HDIM) < half_dim

    def turn(x):
        other = jnp.where(
            lower, pltpu.roll(x, 128 - half_dim, 1), pltpu.roll(x, half_dim, 1)
        )
        return x * cos_ref[...] + other * sin_ref[...]

    pos = lax.broadcasted_iota(jnp.int32, (toks, 128), 0) + sp * toks
    angle = pos.astype(f32) * inv_ref[...]
    cos_ref[...] = jnp.cos(angle)
    sines = jnp.sin(angle)
    sin_ref[...] = jnp.where(lower, -sines, sines)
    both = jnp.concatenate([k_ref[...], v_ref[...]], axis=0).T
    turned = turn(both.astype(f32)).astype(bf)
    kv[WINDOW:, :] = jnp.where(lane_t < HDIM, turned, both)
    pl.semaphore_wait(barrier, n_sp * n_tp)

    sends = []

    def plan(src, dst, ssem, rsem, where):
        c = pltpu.make_async_remote_copy(
            src_ref=src, dst_ref=dst, send_sem=ssem, recv_sem=rsem,
            device_id=where, device_id_type=MESH,
        )
        sends.append(c)
        return c

    def post(src, dst, ssem, rsem, where):
        c = plan(src, dst, ssem, rsem, where)
        c.start()
        return c

    def pool_at(src, dst, group, rsem, where):
        c = pltpu.make_async_remote_copy(
            src_ref=src, dst_ref=dst, send_sem=gss.at[group], recv_sem=rsem,
            device_id=where, device_id_type=MESH,
        )
        c.start()
        return c

    def pool(src, dst, group, rsem, d, k):
        return pool_at(src, dst, group, rsem, {"sp": sp_at(d), "tp": tp_at(k)})

    def send(src, dst, ssem, rsem, d, k):
        return post(src, dst, ssem, rsem, {"sp": sp_at(d), "tp": tp_at(k)})

    tail = post(
        kv.at[pl.ds(toks, WINDOW)], kv.at[pl.ds(0, WINDOW)], kss, krs,
        {"sp": lax.rem(sp + 1, n_sp)},
    )
    chunk = depth // (2 * PIECES)

    def w_rows(k, half, c):
        return pl.ds(pl.multiple_of(k * depth + half * (depth // 2) + c * chunk, chunk), chunk)

    w_far = []

    def w_open(c):
        w_far.append(
            pool(wbuf.at[w_rows(0, grp, c)], wbuf.at[w_rows(2, grp, c)], 2, wrs.at[0, c], 0, 2)
        )

    w_side, w_last = [], []

    def w_cross(c):
        w_far[c].wait_recv()
        mine = wbuf.at[w_rows(2, grp, c)]
        w_side.append(pool_at(mine, mine, 2, wrs.at[1, c], {"grp": 1 - grp}))
        w_last.append(pool(mine, wbuf.at[w_rows(3, grp, c)], 2, wrs.at[2, c], 0, 1))

    def w_close(c):
        w_side[c].wait_recv()
        w_last.append(
            pool(
                wbuf.at[w_rows(2, 1 - grp, c)], wbuf.at[w_rows(3, 1 - grp, c)], 2, wrs.at[3, c], 0, 1
            )
        )

    local[0].wait()
    for c in range(EARLY):
        w_open(c)
    w_near = send(w_at(0), w_at(1), wss, wnr, 0, 1)

    ii = lax.broadcasted_iota(jnp.int32, (rows, rows), 0)
    jj = lax.broadcasted_iota(jnp.int32, (rows, rows), 1)
    low = jnp.where(jj < ii, 1.0, 0.0).astype(bf)
    upp = jnp.where(ii < jj, 1.0, 0.0).astype(bf)

    def relative(first):
        return lax.bitwise_xor(first, jnp.broadcast_to(sp * epg, first.shape))

    lane = lax.broadcasted_iota(jnp.int32, (rows, 128), 1)
    rel_r = relative(routes_t_ref[0:1, :])
    rel_r2 = relative(routes_t_ref[1:2, :])
    rel_c = jnp.sum(jnp.where(ii == jj, rel_r, 0), axis=1, keepdims=True)
    hot_c = jnp.where((rel_c >= lane * epg) & (rel_c < (lane + 1) * epg), 1.0, 0.0)
    rank_c = jnp.dot(low, hot_c.astype(bf), preferred_element_type=f32)
    lane_f = lane.astype(f32)
    slot_c = jnp.sum(hot_c * (lane_f * cap + rank_c), axis=1, keepdims=True)
    wide_c = jnp.sum(hot_c * (lane_f * 128 + rank_c), axis=1, keepdims=True)
    lane_s = lax.broadcasted_iota(jnp.int32, (rows, n_sp * cap), 1).astype(f32)
    pt_ref[...] = jnp.where(lane_s == slot_c, 1.0, 0.0).astype(bf)
    lane_w = lax.broadcasted_iota(jnp.int32, (rows, n_sp * 128), 1).astype(f32)
    pt_wide = jnp.where(lane_w == wide_c, 1.0, 0.0).astype(bf)

    sub = lax.broadcasted_iota(jnp.int32, (16, rows), 0)
    sub_f = sub.astype(f32)
    hot_r = jnp.where((rel_r >= sub * epg) & (rel_r < (sub + 1) * epg), 1.0, 0.0)
    rank_r = jnp.dot(hot_r.astype(bf), upp, preferred_element_type=f32)
    slot_r = jnp.sum(hot_r * (sub_f * cap + rank_r), axis=0, keepdims=True)
    group_r = jnp.sum(hot_r * sub_f, axis=0, keepdims=True)
    sub_s = lax.broadcasted_iota(jnp.int32, (cap, rows), 0).astype(f32)

    def chosen(d):
        return jnp.where(sub_s + float(d * cap) == slot_r, 1.0, 0.0).astype(bf)

    far = {}

    def send_rows(d):
        picked = jnp.dot(chosen(d), res_ref[...], preferred_element_type=f32).astype(bf)
        if d == 0:
            own_r[0] = picked
            return
        if d == LAST:
            rres[d] = picked
            return
        xs[d] = picked
        far[0, d] = send(xs.at[d], rres.at[d], zss.at[0, d], zrs.at[0, d], d, 0)

    own = {}

    def own_cast(kind, src, dst, via):
        buf = own_a if kind else own_r
        own[kind, dst] = send(
            buf.at[src], buf.at[dst], oss.at[kind, dst], ors.at[kind, dst], 0, via
        )

    send_rows(1)
    send_rows(2)
    send_rows(0)
    own_cast(0, 0, 1, 1)

    for j in range(q_ref.shape[1] // 128):
        cs = pl.ds(j * 128, 128)
        rq[:, cs] = turn(q_ref[:, cs].astype(f32)).astype(bf)

    first_r = rel_r.astype(f32) - epg * group_r
    second_r = rel_r2.astype(f32) - epg * group_r
    w_t = jnp.where(first_r == sub_f, rw_t_ref[0:1, :], 0.0) + jnp.where(
        second_r == sub_f, rw_t_ref[1:2, :], 0.0
    )
    hi = w_t.astype(bf)
    rest = w_t - hi.astype(f32)
    mid = rest.astype(bf)
    lo = (rest - mid.astype(f32)).astype(bf)
    placed = (
        jnp.dot(hi, pt_wide, preferred_element_type=f32)
        + jnp.dot(mid, pt_wide, preferred_element_type=f32)
        + jnp.dot(lo, pt_wide, preferred_element_type=f32)
    )
    for d in range(n_sp):
        meta[d] = placed[0:8, d * 128 : (d + 1) * 128]
    meta_rx[0, 0] = placed[0:8, 0:128]
    metas = {}
    for d in range(n_sp):
        for k in range(n_tp):
            if d or k:
                metas[d, k] = send(
                    meta.at[d], meta_rx.at[d, k], mss.at[d, k], mrs.at[d, k], d, k
                )

    n_heads = q_ref.shape[1] // HDIM
    tail.wait_recv()
    qi = lax.broadcasted_iota(jnp.int32, (WINDOW, 2 * WINDOW), 0)
    ki = lax.broadcasted_iota(jnp.int32, (WINDOW, 2 * WINDOW), 1)
    band = (ki > qi) & (ki <= qi + WINDOW)

    def attend(k):
        n = tp_at(k)
        start = pl.multiple_of(n * WINDOW, WINDOW)
        keys = kv[pl.ds(start, 2 * WINDOW), 0:HDIM]
        vals = kv[pl.ds(start, 2 * WINDOW), HDIM : 2 * HDIM]
        q = rq[pl.ds(start, WINDOW), :]
        first = jnp.where((sp == 0) & (n == 0), WINDOW, 0)
        seen = band & (ki >= first)
        outs = []
        for h in range(n_heads):
            sc = lax.dot_general(
                q[:, h * HDIM : (h + 1) * HDIM], keys, (((1,), (1,)), ((), ())),
                preferred_element_type=f32,
            ) * HDIM ** (-0.5)
            sc = jnp.where(seen, sc, -jnp.inf)
            sink = sink_ref[0:1, h : h + 1]
            top = jnp.maximum(jnp.max(sc, axis=1, keepdims=True), sink)
            e = jnp.exp(sc - top)
            den = jnp.sum(e, axis=1, keepdims=True) + jnp.exp(sink - top)
            pr = (e * (1.0 / den)).astype(bf)
            outs.append(jnp.dot(pr, vals, preferred_element_type=f32))
        heads_v[k] = jnp.concatenate(outs, axis=1).astype(bf)

    heads = {}

    def send_heads(k):
        heads[k] = send(heads_v.at[k], abuf.at[k], ass_.at[k], ars.at[k], 0, k)

    tile = width // 4

    def project(d):
        def step(i, _):
            cols = pl.ds(pl.multiple_of(i * tile, tile), tile)
            acc[:, cols] = jnp.dot(rat[d], wbuf[:, cols], preferred_element_type=f32)
            return 0

        lax.fori_loop(0, 4, step, 0)

    def pack_heads(k):
        block = abuf[k] if k else heads_v[0]
        cs = pl.ds(k * depth, depth)
        for d in ORDER:
            picked = jnp.dot(chosen(d), block, preferred_element_type=f32).astype(bf)
            if d == LAST:
                rat[d, :, cs] = picked
            elif d:
                aps[d, :, cs] = picked
            else:
                own_a[0, :, cs] = picked

    def send_heads_far(d):
        far[1, d] = send(aps.at[d], rat.at[d], zss.at[1, d], zrs.at[1, d], d, 0)

    attend(2)
    send_heads(2)
    w_cross(0)
    attend(3)
    send_heads(3)
    for c in range(EARLY, PIECES):
        w_open(c)
    own_cast(0, 0, 2, 2)
    w_cross(1)
    attend(1)
    send_heads(1)
    w_cross(2)
    w_close(0)
    attend(0)
    w_cross(3)
    w_close(1)
    pack_heads(0)
    heads[1].wait_recv()
    pack_heads(1)
    w_close(2)
    heads[2].wait_recv()
    pack_heads(2)
    heads[3].wait_recv()
    pack_heads(3)
    send_heads_far(1)
    send_heads_far(2)
    own_cast(1, 0, 1, 1)
    own_cast(1, 0, 2, 2)
    send_rows(LAST)
    w_near.wait_recv()
    w_cross(4)
    w_close(3)
    w_cross(5)
    w_cross(6)
    w_cross(7)
    w_close(4)
    w_close(5)
    w_close(6)
    w_close(7)
    for c in w_last:
        c.wait_recv()

    def shift(kind, _):
        own[kind, 2].wait_recv()
        own_cast(kind, 2, 3, 1)

    def gather(_, __):
        for kind in range(2):
            own[kind, 1].wait_recv()
            own[kind, 3].wait_recv()

        def step(t, _):
            cols = pl.ds(pl.multiple_of(t * tile, tile), tile)
            left = [
                jnp.concatenate(
                    [own_a[k, :, (i ^ k) * depth : ((i ^ k) + 1) * depth] for i in range(n_tp)], axis=1
                )
                for k in range(n_tp)
            ]
            acc0[:, cols] = jnp.dot(
                jnp.concatenate(left, axis=0), wbuf[:, cols], preferred_element_type=f32
            )
            return 0

        lax.fori_loop(0, 4, step, 0)
        for k in range(n_tp):
            settle(0, k, own_r[k], acc0[k * cap : (k + 1) * cap])

    def settle(d, k, rest, total):
        stream = (rest.astype(f32) + total).astype(bf)
        if k == 0:
            stream_v[d] = stream
        stream_f = stream.astype(f32)
        scale = lax.rsqrt(jnp.mean(stream_f * stream_f, axis=-1, keepdims=True) + norm_eps)
        normed = (stream_f * scale * gain_ref[...]).astype(bf)
        if d == LAST:
            xs[d] = normed
        else:
            tok[d, k] = normed

    ready = {}

    def norm_far(d, _):
        project(d)
        settle(d, 0, rres[d], acc[...])
        for h in range(PARTS):
            ready[h] = pool(xs.at[d, :, part(h)], tok.at[d, 0, :, part(h)], 0, drs.at[0, d, h], d, 0)

    def pass_on(d, h):
        ready[h].wait_recv()
        cast(0, 2, d, h, 2)
        cast(0, 1, d, h, 1)

    half_w = width // PARTS

    def part(h):
        return pl.ds(h * half_w, half_w)

    plane = {}

    def cast(src, dst, d, h, via):
        plane[dst, d, h] = pool(
            tok.at[d, src, :, part(h)], tok.at[d, dst, :, part(h)], 1, drs.at[dst, d, h], 0, via
        )

    def spread(d, _):
        far[0, d].wait_recv()
        far[1, d].wait_recv()
        project(d)
        settle(d, 0, rres[d], acc[...])
        for h in range(PARTS):
            cast(0, 2, d, h, 2)
            cast(0, 1, d, h, 1)

    def relay(d, h):
        plane[2, d, h].wait_recv()
        cast(2, 3, d, h, 1)

    eye = lax.broadcasted_iota(jnp.int32, (cap, 128), 0) == lax.broadcasted_iota(
        jnp.int32, (cap, 128), 1
    )
    f_tile = ff // 2
    back = {}

    def serve(d, _):
        cols = []
        if d:
            for h in range(PARTS):
                plane[1, d, h].wait_recv()
                plane[3, d, h].wait_recv()
        for k in range(n_tp):
            if d or k:
                metas[d, k].wait_recv()
            row = meta_rx[d, k, pl.ds(tp, 1), :]
            cols.append(jnp.sum(jnp.where(eye, row, 0.0), axis=1, keepdims=True))
        weight = jnp.concatenate(cols, axis=0)

        def inner(i, _):
            cs = pl.ds(pl.multiple_of(i * f_tile, f_tile), f_tile)
            x = tok[d].reshape(n_tp * cap, width)
            g = jnp.dot(x, gate_v[:, cs], preferred_element_type=f32)
            u = jnp.dot(x, up_v[:, cs], preferred_element_type=f32)
            hid[:, cs] = (g / (1.0 + jnp.exp(-g)) * u * weight).astype(bf)
            return 0

        lax.fori_loop(0, 2, inner, 0)
        def outer(i, _):
            cs = pl.ds(pl.multiple_of(i * tile, tile), tile)
            o = jnp.dot(hid[...], down_v[:, cs], preferred_element_type=f32).astype(bf)
            y[d, :, :, cs] = o.reshape(n_tp, cap, tile)
            return 0

        per = 4 // PARTS
        for h in range(PARTS):
            lax.fori_loop(h * per, (h + 1) * per, outer, 0)
            for k, slot in ((3, 1), (1, 0)):
                back[k, d, h] = pool(
                    y.at[d, k, :, part(h)], yr.at[d, slot, :, part(h)], 0, rrs.at[slot, d, h], 0, 1
                )

    def pair(d, h):
        cs = part(h)
        back[3, d, h].wait_recv()
        sum2[d, :, cs] = (y[d, 2, :, cs].astype(f32) + yr[d, 1, :, cs].astype(f32)).astype(bf)
        back[2, d, h] = pool(sum2.at[d, :, cs], xrec.at[d, :, cs], 0, rrs.at[2, d, h], 0, 2)
        back[1, d, h].wait_recv()
        sum0[d, :, cs] = y[d, 0, :, cs].astype(f32) + yr[d, 0, :, cs].astype(f32)

    home = {}

    def finish(d, h):
        cs = part(h)
        back[2, d, h].wait_recv()
        total = sum0[d, :, cs] + xrec[d, :, cs].astype(f32)
        if d != LAST:
            total = total + stream_v[d, :, cs].astype(f32)
        total = total.astype(bf)
        if d:
            zsend[d, :, cs] = total
            home[d, h] = pool(zsend.at[d, :, cs], zrec.at[d, :, cs], 0, rrs.at[3, d, h], d, 0)
        else:
            zrec[0, :, cs] = total

    inner_steps = (
        (spread, 2, 0),
        (norm_far, 3, 0),
        (spread, 1, 0),
        (shift, 0, 0),
        (shift, 1, 0),
        (gather, 0, 0),
        (relay, 2, 0),
        (relay, 2, 1),
        (relay, 2, 2),
        (relay, 2, 3),
        (serve, 2, 0),
        (pair, 2, 0),
        (pair, 2, 1),
        (pair, 2, 2),
        (pair, 2, 3),
        (relay, 1, 0),
        (relay, 1, 1),
        (relay, 1, 2),
        (relay, 1, 3),
        (pass_on, 3, 0),
        (pass_on, 3, 1),
        (pass_on, 3, 2),
        (pass_on, 3, 3),
        (serve, 1, 0),
        (pair, 1, 0),
        (pair, 1, 1),
        (pair, 1, 2),
        (pair, 1, 3),
        (finish, 2, 0),
        (finish, 2, 1),
        (serve, 0, 0),
        (finish, 2, 2),
        (finish, 2, 3),
        (relay, 3, 0),
        (relay, 3, 1),
        (relay, 3, 2),
        (relay, 3, 3),
        (serve, 3, 0),
        (pair, 3, 0),
        (finish, 1, 0),
        (pair, 3, 1),
        (finish, 1, 1),
        (pair, 3, 2),
        (finish, 1, 2),
        (pair, 3, 3),
        (finish, 1, 3),
        (pair, 0, 0),
        (finish, 3, 0),
        (pair, 0, 1),
        (finish, 3, 1),
        (pair, 0, 2),
        (finish, 3, 2),
        (pair, 0, 3),
        (finish, 3, 3),
        (finish, 0, 0),
        (finish, 0, 1),
        (finish, 0, 2),
        (finish, 0, 3),
    )
    outer_steps = (
        (spread, 2, 0),
        (norm_far, 3, 0),
        (spread, 1, 0),
        (shift, 0, 0),
        (shift, 1, 0),
        (gather, 0, 0),
        (relay, 2, 0),
        (relay, 2, 1),
        (relay, 2, 2),
        (relay, 2, 3),
        (serve, 2, 0),
        (pass_on, 3, 0),
        (pass_on, 3, 1),
        (pass_on, 3, 2),
        (pass_on, 3, 3),
        (pair, 2, 0),
        (pair, 2, 1),
        (pair, 2, 2),
        (pair, 2, 3),
        (relay, 1, 0),
        (relay, 1, 1),
        (relay, 1, 2),
        (relay, 1, 3),
        (serve, 1, 0),
        (relay, 3, 0),
        (relay, 3, 1),
        (relay, 3, 2),
        (relay, 3, 3),
        (serve, 3, 0),
        (finish, 2, 0),
        (finish, 2, 1),
        (pair, 3, 0),
        (pair, 3, 1),
        (pair, 3, 2),
        (pair, 3, 3),
        (finish, 2, 2),
        (finish, 2, 3),
        (pair, 1, 0),
        (pair, 1, 1),
        (pair, 1, 2),
        (pair, 1, 3),
        (finish, 3, 0),
        (serve, 0, 0),
        (finish, 3, 1),
        (finish, 3, 2),
        (finish, 3, 3),
        (pair, 0, 0),
        (pair, 0, 1),
        (pair, 0, 2),
        (pair, 0, 3),
        (finish, 1, 0),
        (finish, 1, 1),
        (finish, 1, 2),
        (finish, 1, 3),
        (finish, 0, 0),
        (finish, 0, 1),
        (finish, 0, 2),
        (finish, 0, 3),
    )
    for c in local[1:]:
        c.wait()

    def close(i, _):
        cs = pl.ds(pl.multiple_of(i * tile, tile), tile)
        last = (zrec[LAST, :, cs].astype(f32) + stream_v[LAST, :, cs].astype(f32)).astype(bf)
        rec = jnp.concatenate([zrec[d, :, cs] for d in range(LAST)] + [last], axis=0)
        got = jnp.dot(pt_ref[...], rec, preferred_element_type=f32)
        out_ref[:, cs] = got.astype(bf)
        return 0

    def rest(steps):
        before = list(sends)
        for stage, d, h in steps:
            stage(d, h)
        for h in range(PARTS):
            for d in ORDER[1:]:
                home[d, h].wait_recv()
            lax.fori_loop(h * 4 // PARTS, (h + 1) * 4 // PARTS, close, 0)
        for c in sends:
            c.wait_send()
        spans = (
            tok, tok.at[pl.ds(0, n_sp - 1), pl.ds(0, n_tp - 1)], wbuf.at[pl.ds(0, 2 * depth)],
        )
        for group, span in enumerate(spans):
            pltpu.make_async_remote_copy(
                src_ref=span, dst_ref=span, send_sem=gss.at[group], recv_sem=krs,
                device_id={"sp": sp_at(1), "tp": tp_at(0)}, device_id_type=MESH,
            ).wait_send()
        sends[:] = before

    inner = (sp == 1) | (sp == n_sp - 2)
    pl.when(inner)(functools.partial(rest, inner_steps))
    pl.when(jnp.logical_not(inner))(functools.partial(rest, outer_steps))


def whole_layer(
    query_rows, key_rows, value_rows, sink_logits, residual, out_weight, norm_gain, gate_weight, up_weight, down_weight, routes,
    route_weight,
):
    n_tp = lax.axis_size("tp")
    n_sp = lax.axis_size("sp")
    rows, width = residual.shape
    ff = gate_weight.shape[2]
    depth = out_weight.shape[0]
    cap = 2 * rows // n_sp
    toks = query_rows.shape[0]
    half_dim = HDIM // 2
    inverse = rope_base ** (-np.arange(half_dim, dtype=np.float32) / np.float32(half_dim))
    table = np.tile(inverse.astype(np.float32), 4)[None, :]
    bf = jnp.bfloat16
    f32 = jnp.float32
    dma = pltpu.SemaphoreType.DMA
    vm = pl.BlockSpec(memory_space=pltpu.VMEM)
    hbm = pl.BlockSpec(memory_space=pl.ANY)
    return pl.pallas_call(
        layer_kernel,
        out_shape=jax.ShapeDtypeStruct((rows, width), bf),
        in_specs=[vm] * 5 + [hbm, vm, vm, vm, vm, hbm, hbm, hbm],
        out_specs=vm,
        scratch_shapes=[
            pltpu.VMEM((n_tp * depth, width), bf),
            pltpu.VMEM((n_tp, rows, depth), bf),
            pltpu.VMEM((cap, width), f32),
            pltpu.VMEM((n_sp, cap, width), bf),
            pltpu.VMEM((n_sp, cap, width), bf),
            pltpu.VMEM((n_sp, cap, n_tp * depth), bf),
            pltpu.VMEM((n_sp, cap, n_tp * depth), bf),
            pltpu.VMEM((n_tp, cap, width), bf),
            pltpu.VMEM((n_tp, cap, n_tp * depth), bf),
            pltpu.VMEM((n_tp * cap, width), f32),
            pltpu.VMEM((n_sp, n_tp, cap, width), bf),
            pltpu.VMEM((width, ff), bf),
            pltpu.VMEM((width, ff), bf),
            pltpu.VMEM((ff, width), bf),
            pltpu.VMEM((n_tp * cap, ff), bf),
            pltpu.VMEM((n_sp, n_tp, cap, width), bf),
            pltpu.VMEM((n_sp, 2, cap, width), bf),
            pltpu.VMEM((n_sp, cap, width), f32),
            pltpu.VMEM((n_sp, cap, width), bf),
            pltpu.VMEM((n_sp, cap, width), bf),
            pltpu.VMEM((n_sp, cap, width), bf),
            pltpu.VMEM((n_sp, cap, width), bf),
            pltpu.VMEM((n_sp, 8, 128), f32),
            pltpu.VMEM((n_sp, n_tp, 8, 128), f32),
            pltpu.VMEM((rows, n_sp * cap), bf),
            pltpu.VMEM((n_sp, cap, width), bf),
            pltpu.VMEM((toks + WINDOW, 2 * HDIM), bf),
            pltpu.VMEM((toks, depth), bf),
            pltpu.VMEM((n_tp, rows, depth), bf),
            pltpu.VMEM((toks, 128), f32),
            pltpu.VMEM((toks, 128), f32),
            dma((4,)), dma, dma, dma((4, PIECES)), dma, dma, dma((4,)), dma((4,)),
            dma((n_sp, n_tp)), dma((n_sp, n_tp)), dma((2, n_sp)), dma((2, n_sp)),
            dma((2, n_tp)), dma((2, n_tp)),
            dma((3,)), dma((4, n_sp, PARTS)), dma((4, n_sp, PARTS)),
        ],
        compiler_params=pltpu.CompilerParams(
            collective_id=0, has_side_effects=True, vmem_limit_bytes=60000 * 1024
        ),
        name="routed_layer",
    )(
        query_rows, key_rows.T, value_rows.T, jnp.asarray(table), sink_logits[None, :],
        out_weight,
        residual, norm_gain[None, :],
        routes.T, route_weight.T, gate_weight[0], up_weight[0], down_weight[0],
    )


def per_device(
    query_rows,
    key_rows,
    value_rows,
    sink_logits,
    residual,
    out_weight,
    norm_gain,
    gate_weight,
    up_weight,
    down_weight,
    routes,
    route_weight,
):
    tok_count = query_rows.shape[0]
    fits = (
        lax.axis_size("grp") == 2
        and lax.axis_size("sp") == GROUPS
        and lax.axis_size("tp") == 4
        and residual.shape[0] == WINDOW
        and key_rows.shape[1] == HDIM
        and query_rows.shape[1] % 128 == 0
    )
    if fits:
        return whole_layer(
            query_rows, key_rows, value_rows, sink_logits, residual, out_weight, norm_gain,
            gate_weight, up_weight, down_weight, routes, route_weight,
        )
    head_local = query_rows.shape[1] // HDIM
    group_local = key_rows.shape[1] // HDIM
    repeat = head_local // group_local
    first_pos = lax.axis_index("sp") * tok_count
    positions = first_pos + jnp.arange(tok_count, dtype=jnp.int32)
    rot_q = rotate(query_rows, positions, head_local)
    rot_k = rotate(key_rows, positions, group_local)
    tails = jnp.stack([rot_k[tok_count - WINDOW :], value_rows[tok_count - WINDOW :]])
    earlier = shifted(tails, "sp", 1)
    blocks = tok_count // WINDOW
    q_blocks = rot_q.reshape(blocks, WINDOW, group_local, repeat, HDIM)
    k_blocks = rot_k.reshape(blocks, WINDOW, group_local, HDIM)
    v_blocks = value_rows.reshape(blocks, WINDOW, group_local, HDIM)
    k_prev = jnp.concatenate(
        [earlier[0].reshape(1, WINDOW, group_local, HDIM), k_blocks[:-1]], axis=0
    )
    v_prev = jnp.concatenate(
        [earlier[1].reshape(1, WINDOW, group_local, HDIM), v_blocks[:-1]], axis=0
    )
    k_wide = jnp.concatenate([k_prev, k_blocks], axis=1)
    v_wide = jnp.concatenate([v_prev, v_blocks], axis=1)
    query_pos = jnp.arange(WINDOW) + WINDOW
    key_pos = jnp.arange(2 * WINDOW)
    distance = query_pos[:, None] - key_pos[None, :]
    in_band = (distance >= 0) & (distance < WINDOW)
    key_global = (
        first_pos + jnp.arange(blocks)[:, None, None] * WINDOW + key_pos[None, None, :] - WINDOW
    )
    allowed = in_band[None] & (key_global >= 0)
    scores = jnp.einsum(
        "nqgrd,nkgd->grnqk", q_blocks, k_wide, preferred_element_type=jnp.float32
    ) * HDIM ** (-0.5)
    scores = jnp.where(allowed[None, None], scores, -jnp.inf)
    sink_here = sink_logits.reshape(group_local, repeat)[:, :, None, None, None]
    largest = jnp.maximum(scores.max(axis=-1, keepdims=True), sink_here)
    exp_scores = jnp.exp(scores - largest)
    denominator = exp_scores.sum(axis=-1, keepdims=True) + jnp.exp(sink_here - largest)
    probs = (exp_scores / denominator).astype(jnp.bfloat16)
    attended = jnp.einsum("grnqk,nkgd->nqgrd", probs, v_wide, preferred_element_type=jnp.float32)
    attended = attended.astype(jnp.bfloat16).reshape(tok_count, head_local * HDIM)
    row_count = residual.shape[0]
    token_rows = lax.all_to_all(attended, "tp", split_axis=0, concat_axis=1, tiled=True)
    projected = jnp.dot(
        token_rows,
        lax.all_gather(out_weight, "tp", axis=0, tiled=True),
        preferred_element_type=jnp.float32,
    )
    stream_f = (residual.astype(jnp.float32) + projected).astype(jnp.bfloat16).astype(jnp.float32)
    normed = (
        stream_f
        * lax.rsqrt(jnp.mean(stream_f * stream_f, axis=-1, keepdims=True) + norm_eps)
        * norm_gain[None, :]
    ).astype(jnp.bfloat16)
    sp_count = lax.axis_size("sp")
    tp_count = lax.axis_size("tp")
    expert_count = sp_count * tp_count
    capacity = 4 * row_count // expert_count
    width = normed.shape[1]
    flat_expert = routes.reshape(-1)
    one_hot = (flat_expert[:, None] == jnp.arange(expert_count, dtype=jnp.int32)[None, :]).astype(
        jnp.int32
    )
    slot_rank = jnp.sum((jnp.cumsum(one_hot, axis=0) - one_hot) * one_hot, axis=1)
    slot_index = flat_expert * capacity + slot_rank
    token_of = jnp.arange(2 * row_count, dtype=jnp.int32) // 2
    outgoing = (
        jnp.zeros((expert_count * capacity, width), jnp.bfloat16)
        .at[slot_index]
        .set(normed[token_of])
    )
    outgoing = outgoing.reshape(expert_count, capacity, width)
    arrived = lax.all_to_all(outgoing, ("sp", "tp"), split_axis=0, concat_axis=0, tiled=True)
    flat_rows = arrived.reshape(-1, width)
    gate_out = jnp.dot(flat_rows, gate_weight[0], preferred_element_type=jnp.float32)
    up_out = jnp.dot(flat_rows, up_weight[0], preferred_element_type=jnp.float32)
    hidden = (jax.nn.silu(gate_out) * up_out).astype(jnp.bfloat16)
    produced = jnp.dot(hidden, down_weight[0], preferred_element_type=jnp.float32).astype(
        jnp.bfloat16
    )
    returned = lax.all_to_all(
        produced.reshape(arrived.shape), ("sp", "tp"), split_axis=0, concat_axis=0, tiled=True
    )
    gathered = returned.reshape(expert_count * capacity, width)[slot_index].astype(jnp.float32)
    weighted = gathered * route_weight.reshape(-1)[:, None]
    combined = weighted.reshape(row_count, 2, width).sum(axis=1)
    return (stream_f + combined).astype(jnp.bfloat16)


def solution(mesh):
    in_specs = (
        P(("grp", "sp"), "tp"),
        P(("grp", "sp"), "tp"),
        P(("grp", "sp"), "tp"),
        P("tp"),
        P(("grp", "sp", "tp"), None),
        P("tp", None),
        P(),
        P(("sp", "tp"), None, None),
        P(("sp", "tp"), None, None),
        P(("sp", "tp"), None, None),
        P(("grp", "sp", "tp"), None),
        P(("grp", "sp", "tp"), None),
    )
    out_specs = P(("grp", "sp", "tp"), None)
    return jax.shard_map(
        per_device, mesh=mesh, in_specs=in_specs, out_specs=out_specs, check_vma=False
    )
```
